256 devices in a mesh: sp: 64 (over z, y, core), tp: 4 (over x).
Axes of the slice: x: 4, y: 4, z: 8, core: 2. Of those that a mesh axis runs over, the one named last changes fastest.
Arguments:
- head_input_values: bfloat16 [24576, 4096], P('sp', 'tp'), may hold values from -6 to 6
- group_input_vectors: bfloat16 [24576, 1024], P('sp', 'tp'), may hold values from -6 to 6
- group_readout_vectors: bfloat16 [24576, 1024], P('sp', 'tp'), may hold values from -6 to 6
- output_gate_values: bfloat16 [24576, 4096], P('sp', 'tp'), may hold values from -6 to 6
- step_size_logits: float32 [24576, 64], P('sp', 'tp'), may hold values from -6 to 6
- extra_log_decay: float32 [24576, 64], P('sp', 'tp'), may hold values from -1.2 to 0
- head_input_filter: bfloat16 [4, 4096], P(None, 'tp'), may hold values from -3 to 3
- input_vector_filter: bfloat16 [4, 1024], P(None, 'tp'), may hold values from -3 to 3
- readout_vector_filter: bfloat16 [4, 1024], P(None, 'tp'), may hold values from -3 to 3
- step_size_bias: float32 [64], P('tp'), may hold values from -0.5 to 0.5
- head_rate_logarithm: float32 [64], P('tp'), may hold values from -20 to -1
- direct_path_weight: float32 [64], P('tp'), may hold values from 0 to 3
- group_norm_scale: bfloat16 [4096], P('tp'), may hold values from 0.099609375 to 1.8984375
- mixer_output_weight: bfloat16 [4096, 2048], P('tp'), may hold values from -0.09375 to 0.09375
- residual: bfloat16 [24576, 2048], P(('sp', 'tp')), may hold values from -6 to 6
- first_norm_scale: float32 [2048], replicated, may hold values from 0.1 to 1.9
- first_norm_bias: float32 [2048], replicated, may hold values from -1.5 to 1.5
- routes: int32 [24576, 2], P(('sp', 'tp')), may hold values from 0 to 63, all different within a row; in each aligned block of 96 rows (0 to 95, 96 to 191, ...) at most 5 rows name the same one
- routing_weight: float32 [24576, 2], P(('sp', 'tp')), may hold values from 0.1 to 0.9
- expert_gate_weight: bfloat16 [64, 2048, 1024], P('sp', None, 'tp'), may hold values from -0.125 to 0.125
- expert_up_weight: bfloat16 [64, 2048, 1024], P('sp', None, 'tp'), may hold values from -0.125 to 0.125
- expert_down_weight: bfloat16 [64, 2048, 1024], P('sp', None, 'tp'), may hold values from -0.1875 to 0.1875
- final_norm_scale: float32 [2048], replicated, may hold values from 0.1 to 1.9
- final_norm_bias: float32 [2048], replicated, may hold values from -1.5 to 1.5
Outputs:
- final: bfloat16 [24576, 2048], P(('sp', 'tp'))
The draws below stay inside these ranges and needn't reach their ends.
Inputs may be any that keep to these rules, and one draw needn't show every extreme that they name: `routes`: in the rows of one device no expert is named more than 5 times.
All inputs are finite; a program needn't handle non-finite values.
Results may differ from the reference program's by a relative error of at most 0.012.
Values may be sent and summed in bfloat16 or wider, within the bound.
No kernel may reach another device: no remote copies, remote signals or barrier semaphores. Data moves between devices by JAX's collectives and lax.ppermute only.
A program may use at most 128 MiB of HBM per device.

```python
import math
import jax
import jax.numpy as jnp
import numpy as np
from jax import lax

D = 2048
HEAD_COUNT = 64
HEAD_DIM = 64
INNER_WIDTH = 4096
GROUP_COUNT = 8
STATE_WIDTH = 128
TAPS = 4
BLOCK_LENGTH = 128
FFE = 1024
TOPK = 2
EXPERTS = 64
TOK_DEV = 384
TOKEN_COUNT = 24576
CAP = 5
N_SP = 64
N_TP = 4


def draw_step_size_logits(key, part):
    key_noise, key_shift, key_heat = jax.random.split(jax.random.fold_in(key, 11), 3)
    block_list = TOKEN_COUNT // TOK_DEV
    heated = jax.random.bernoulli(key_heat, 0.0625, (block_list, 1, HEAD_COUNT))
    jitter = jax.random.uniform(key_shift, (block_list, 1, HEAD_COUNT), jnp.float32, -0.3, 0.3)
    block_shift = jnp.where(heated, 3.5, -1.0) + jitter
    noise_part = 0.7 * jax.random.normal(key_noise, (block_list, TOK_DEV, HEAD_COUNT), jnp.float32)
    return jnp.clip(noise_part + block_shift, -6.0, 6.0).reshape(TOKEN_COUNT, HEAD_COUNT)


def draw_head_rate_logarithm(key, part):
    key_pick, key_fast, key_slow = jax.random.split(jax.random.fold_in(key, 12), 3)
    chance = 0.5
    quick = jax.random.bernoulli(key_pick, chance, (HEAD_COUNT,))
    fast_rate = jnp.log(jax.random.uniform(key_fast, (HEAD_COUNT,), jnp.float32, 0.05, 0.15))
    slow_rate = jnp.log(jax.random.uniform(key_slow, (HEAD_COUNT,), jnp.float32, 0.9, 1.4)) - jnp.log(jnp.float32(0.6 * TOKEN_COUNT))
    return jnp.where(quick, fast_rate, slow_rate)


def draw_extra_log_decay(key, part):
    random_key_split, key_depth = jax.random.split(jax.random.fold_in(key, 13))
    extra_decay_rows = jax.random.randint(random_key_split, (2, HEAD_COUNT), 0, TOKEN_COUNT)
    cumulative_log_decay = jnp.log(jax.random.uniform(key_depth, (2, HEAD_COUNT), jnp.float32, 0.55, 0.8))
    position_index = jnp.arange(TOKEN_COUNT, dtype=jnp.int32)[:, None]
    summed_output = jnp.zeros((TOKEN_COUNT, HEAD_COUNT), jnp.float32)
    for block_total in range(2):
        summed_output = summed_output + jnp.where(position_index == extra_decay_rows[block_total][None, :], cumulative_log_decay[block_total][None, :], 0.0)
    return summed_output


def level_of(stream_key, extent, cuts, smallest, top_value):
    factor_of = 1.0
    for dim, shards_of in cuts:
        draws = jax.random.uniform(jax.random.fold_in(jax.random.fold_in(stream_key, 6), dim), (shards_of,), jnp.float32, smallest / len(cuts), top_value / len(cuts))
        factor_of = factor_of * jnp.repeat(jnp.exp(draws), extent[dim] // shards_of).reshape((-1,) + (1,) * (len(extent) - 1 - dim))
    return factor_of


def shared_out(key, own, number, rows, count, top, most, lean):
    order = jax.random.permutation(key, count)
    packed, common = load_shares(count, rows * top, most, lean, True), load_shares(count, rows * top, most, lean, False)
    places = jnp.arange(count)

    def named(sizes, turn):
        used = int((sizes > 0).sum())
        fixed = max(1, used // 4)
        passed = fixed + (places - fixed + turn * (used - fixed)) % max(1, count - fixed)
        return jnp.zeros((count,), jnp.int32).at[order[jnp.where(places < fixed, places, passed)]].set(jnp.asarray(sizes, jnp.int32))

    sizes = jnp.where(number % 4 == 0, named(packed, number // 4), named(common, number - number // 4 - 1))
    mixed = jax.random.permutation(jax.random.fold_in(own, 3), count)
    donor, receiver = mixed[0:count // 2 * 2:2], mixed[1:count // 2 * 2:2]
    room = jnp.minimum(sizes[donor] - 1, most - sizes[receiver]) // 2
    room = jnp.where((donor == order[0]) | (receiver == order[0]) | (sizes[receiver] == 0), 0, jnp.maximum(room, 0))
    passed = jax.random.randint(jax.random.fold_in(own, 4), (count // 2,), 0, 1 << 20) % (room + 1)
    sizes = sizes.at[donor].add(-passed).at[receiver].add(passed)
    items = jnp.searchsorted(jnp.cumsum(sizes), jnp.arange(rows * top), side="right").astype(jnp.int32)
    listing = items.reshape(top, rows).T
    listing = listing[jax.random.permutation(jax.random.fold_in(own, 1), rows)]
    turn = jax.random.randint(jax.random.fold_in(own, 2), (rows, 1), 0, top)
    return jnp.take_along_axis(listing, (jnp.arange(top)[None, :] + turn) % top, axis=1)


def load_shares(amount, total, reach, skew, full):
    weights = [(1 << 20) // math.isqrt(standing ** skew) + 1 for standing in range(1, amount + 1)]
    largest = reach if full else min(reach, max(-(-total // amount), total * weights[0] // sum(weights)))
    least = 1 if total - largest >= amount - 1 else 0
    counts, surplus = [largest] + [least] * (amount - 1), total - largest - least * (amount - 1)
    while surplus > 0:
        free = [i for i in range(1, amount) if counts[i] < largest] or [i for i in range(1, amount) if counts[i] < reach]
        pool, left = sum([weights[i] for i in free]), surplus
        for i in free:
            more = min(reach - counts[i], max(1, left * weights[i] // pool), surplus)
            counts[i] = counts[i] + more
            surplus = surplus - more
    return np.array(counts)


def noise(own_key, shape, scale, most, shards=(), kind=jnp.bfloat16):
    result = scale * jax.random.normal(own_key, shape, jnp.float32)
    if shards:
        result = result * level_of(own_key, shape, shards, -0.22, 0.18)
    return jnp.clip(result, -most, most).astype(kind)


def setup_inputs(seed: int = 0) -> dict:
    seeds = jax.random.split(jax.random.key(seed), 25)
    head_input_values = noise(seeds[0], (TOKEN_COUNT, INNER_WIDTH), 1.0, 6.0, ((0, 64), (1, 4)))
    group_input_vectors = noise(seeds[1], (TOKEN_COUNT, GROUP_COUNT * STATE_WIDTH), 1.0, 6.0, ((0, 64), (1, 4)))
    group_readout_vectors = noise(seeds[2], (TOKEN_COUNT, GROUP_COUNT * STATE_WIDTH), 1.0, 6.0, ((0, 64), (1, 4)))
    output_gate_values = noise(seeds[3], (TOKEN_COUNT, INNER_WIDTH), 1.0, 6.0, ((0, 64), (1, 4)))
    step_size_logits = draw_step_size_logits(jax.random.fold_in(seeds[24], 71), 0)
    extra_log_decay = draw_extra_log_decay(jax.random.fold_in(seeds[24], 71), 0)
    head_input_filter = noise(seeds[6], (TAPS, INNER_WIDTH), 0.5, 3.0, ((1, 4),))
    input_vector_filter = noise(seeds[7], (TAPS, GROUP_COUNT * STATE_WIDTH), 0.5, 3.0, ((1, 4),))
    readout_vector_filter = noise(seeds[8], (TAPS, GROUP_COUNT * STATE_WIDTH), 0.5, 3.0, ((1, 4),))
    step_size_bias = jnp.clip(jax.random.uniform(seeds[9], (HEAD_COUNT,), jnp.float32, -0.5, 0.5) * level_of(seeds[9], (HEAD_COUNT,), ((0, 4),), -0.4, 0.0), -0.5, 0.5)
    head_rate_logarithm = draw_head_rate_logarithm(jax.random.fold_in(seeds[24], 71), 0)
    direct_path_weight = jnp.clip(3.0 * jax.random.uniform(seeds[11], (HEAD_COUNT,), jnp.float32) ** level_of(seeds[11], (HEAD_COUNT,), ((0, 4),), -0.2, 0.2), 0.0, 3.0)
    group_norm_scale = jnp.clip(1.0 + 0.18 * jax.random.normal(seeds[12], (INNER_WIDTH,), jnp.float32), 0.099609375, 1.8984375).astype(jnp.bfloat16)
    mixer_output_weight = noise(seeds[13], (INNER_WIDTH, D), INNER_WIDTH ** -0.5, 0.09375, ((0, 4),))
    residual = noise(seeds[14], (TOKEN_COUNT, D), 1.0, 6.0, ((0, 256),))
    first_norm_scale = jnp.clip(1.0 + 0.18 * jax.random.normal(seeds[15], (D,), jnp.float32), 0.1, 1.9)
    first_norm_bias = noise(seeds[16], (D,), 0.3, 1.5, (), jnp.float32)
    routes_keys = jax.random.split(jax.random.fold_in(seeds[17], 1), TOKEN_COUNT // (TOK_DEV // N_TP))
    routes_turns = jax.random.permutation(jax.random.fold_in(seeds[17], 3), TOKEN_COUNT // (TOK_DEV // N_TP))
    routes = jax.vmap(lambda own, number: shared_out(jax.random.fold_in(seeds[17], 2), own, number, TOK_DEV // N_TP, EXPERTS, TOPK, CAP, 2))(routes_keys, routes_turns).reshape((TOKEN_COUNT, TOPK))
    routing_weight = jnp.clip(0.1 + 0.79999997 * jax.random.uniform(seeds[18], (TOKEN_COUNT, TOPK), jnp.float32) ** level_of(seeds[18], (TOKEN_COUNT, TOPK), ((0, 256),), -0.2, 0.2), 0.1, 0.9)
    expert_gate_weight = noise(seeds[19], (EXPERTS, D, FFE), D ** -0.5, 0.125, ((0, 64), (2, 4)))
    expert_up_weight = noise(seeds[20], (EXPERTS, D, FFE), D ** -0.5, 0.125, ((0, 64), (2, 4)))
    expert_down_weight = noise(seeds[21], (EXPERTS, D, FFE), FFE ** -0.5, 0.1875, ((0, 64), (2, 4)))
    final_norm_scale = jnp.clip(1.0 + 0.18 * jax.random.normal(seeds[22], (D,), jnp.float32), 0.1, 1.9)
    final_norm_bias = noise(seeds[23], (D,), 0.3, 1.5, (), jnp.float32)
    return dict(head_input_values=head_input_values, group_input_vectors=group_input_vectors, group_readout_vectors=group_readout_vectors, output_gate_values=output_gate_values, step_size_logits=step_size_logits, extra_log_decay=extra_log_decay, head_input_filter=head_input_filter, input_vector_filter=input_vector_filter, readout_vector_filter=readout_vector_filter, step_size_bias=step_size_bias, head_rate_logarithm=head_rate_logarithm, direct_path_weight=direct_path_weight, group_norm_scale=group_norm_scale, mixer_output_weight=mixer_output_weight, residual=residual, first_norm_scale=first_norm_scale, first_norm_bias=first_norm_bias, routes=routes, routing_weight=routing_weight, expert_gate_weight=expert_gate_weight, expert_up_weight=expert_up_weight, expert_down_weight=expert_down_weight, final_norm_scale=final_norm_scale, final_norm_bias=final_norm_bias)


EPS = 1e-05
ALPHA = 8.0 ** 0.25

def layer_norm(values, gain_row, bias_row):
    mean_value = lax.optimization_barrier(jnp.mean(values, axis=-1, keepdims=True))
    centred = values - mean_value
    spread = lax.optimization_barrier(jnp.mean(centred * centred, axis=-1, keepdims=True))
    return centred * lax.rsqrt(spread + EPS) * gain_row + bias_row

def conv_silu(raw_rows, tail_rows, tap_weights):
    full_rows = jnp.concatenate([tail_rows, raw_rows], axis=0).astype(jnp.float32)
    weights = tap_weights.astype(jnp.float32)
    length = raw_rows.shape[0]
    summed_output = jnp.zeros((length, raw_rows.shape[1]), jnp.float32)
    for offset in range(tap_weights.shape[0]):
        summed_output = summed_output + weights[offset] * full_rows[offset:offset + length]
    return jax.nn.silu(summed_output)

def block_pass(state_now, input_blocks):
    step_scaled_inputs, decay_logarithm, inputs_b, reads_c = input_blocks
    running = jnp.cumsum(decay_logarithm, axis=0)
    running_t = jnp.moveaxis(running, 0, -1)
    length = decay_logarithm.shape[0]
    causal = jnp.arange(length)[:, None] >= jnp.arange(length)[None, :]
    spread_log = jnp.where(causal, running_t[..., :, None] - running_t[..., None, :], -jnp.inf)
    decay_factors = jnp.exp(spread_log)
    decay_products = jnp.einsum('tgn,sgn->gts', reads_c, inputs_b, precision=lax.Precision.HIGHEST)
    within_block_output = jnp.einsum('zmka,azmo->kzmo', decay_products[:, None] * decay_factors, step_scaled_inputs, precision=lax.Precision.HIGHEST)
    carried_in = jnp.einsum('tgn,grpn->tgrp', reads_c, state_now, precision=lax.Precision.HIGHEST) * jnp.exp(running)[..., None]
    to_end = jnp.exp(running_t[..., -1:] - running_t)
    added = jnp.einsum('sgn,grs,sgrp->grpn', inputs_b, to_end, step_scaled_inputs, precision=lax.Precision.HIGHEST)
    state_next = jnp.exp(running_t[..., -1])[..., None, None] * state_now + added
    return (state_next, within_block_output + carried_in)

def slot_layout(block_routes, capacity, experts):
    flat_routes = block_routes.reshape(-1)
    matches = (flat_routes[:, None] == jnp.arange(experts, dtype=jnp.int32)[None, :]).astype(jnp.int32)
    before = jnp.cumsum(matches, axis=0) - matches
    return flat_routes * capacity + lax.optimization_barrier(jnp.sum(before * matches, axis=1))

def partial_layout(capacity, experts):

    def layout_one(block_routes):
        return slot_layout(block_routes, capacity, experts)
    return layout_one

def reference(head_input_values, group_input_vectors, group_readout_vectors, output_gate_values, step_size_logits, extra_log_decay, head_input_filter, input_vector_filter, readout_vector_filter, step_size_bias, head_rate_logarithm, direct_path_weight, group_norm_scale, mixer_output_weight, residual, first_norm_scale, first_norm_bias, routes, routing_weight, expert_gate_weight, expert_up_weight, expert_down_weight, final_norm_scale, final_norm_bias):
    repeat_count = HEAD_COUNT // GROUP_COUNT
    margin = TAPS - 1

    def mixer_block(carry, input_blocks):
        state_now, tail_x, tail_b, tail_c = carry
        unmixed_head_inputs, unmixed_input_vectors, unmixed_readout_vectors, unmixed_gate_values, unmixed_step_sizes, extra_decay_rows = input_blocks
        length = unmixed_head_inputs.shape[0]
        conv_x = conv_silu(unmixed_head_inputs, tail_x, head_input_filter)
        conv_b = conv_silu(unmixed_input_vectors, tail_b, input_vector_filter)
        conv_c = conv_silu(unmixed_readout_vectors, tail_c, readout_vector_filter)
        step_sizes = jax.nn.softplus(unmixed_step_sizes + step_size_bias)
        decay_logarithm = -step_sizes * jnp.exp(head_rate_logarithm) + extra_decay_rows
        heads_x = conv_x.reshape(length, GROUP_COUNT, repeat_count, HEAD_DIM)
        step_scaled_inputs = heads_x * step_sizes.reshape(length, GROUP_COUNT, repeat_count)[..., None]
        state_next, ssm_out = block_pass(state_now, (step_scaled_inputs, decay_logarithm.reshape(length, GROUP_COUNT, repeat_count), conv_b.reshape(length, GROUP_COUNT, STATE_WIDTH), conv_c.reshape(length, GROUP_COUNT, STATE_WIDTH)))
        ssm_out = ssm_out + direct_path_weight.reshape(GROUP_COUNT, repeat_count)[None, :, :, None] * heads_x
        gated = ssm_out.reshape(length, INNER_WIDTH) * jax.nn.silu(unmixed_gate_values.astype(jnp.float32))
        grouped = gated.reshape(length, GROUP_COUNT, -1)
        normed = grouped * lax.rsqrt(lax.optimization_barrier(jnp.mean(grouped * grouped, axis=-1, keepdims=True)) + EPS)
        rows_out = (normed.reshape(length, INNER_WIDTH) * group_norm_scale.astype(jnp.float32)).astype(jnp.bfloat16)
        return ((state_next, unmixed_head_inputs[length - margin:], unmixed_input_vectors[length - margin:], unmixed_readout_vectors[length - margin:]), rows_out)
    block_list = TOKEN_COUNT // BLOCK_LENGTH
    start = (jnp.zeros((GROUP_COUNT, repeat_count, HEAD_DIM, STATE_WIDTH), jnp.float32), jnp.zeros((margin, INNER_WIDTH), jnp.bfloat16), jnp.zeros((margin, GROUP_COUNT * STATE_WIDTH), jnp.bfloat16), jnp.zeros((margin, GROUP_COUNT * STATE_WIDTH), jnp.bfloat16))
    scan_results = (head_input_values.reshape(block_list, BLOCK_LENGTH, INNER_WIDTH), group_input_vectors.reshape(block_list, BLOCK_LENGTH, GROUP_COUNT * STATE_WIDTH), group_readout_vectors.reshape(block_list, BLOCK_LENGTH, GROUP_COUNT * STATE_WIDTH), output_gate_values.reshape(block_list, BLOCK_LENGTH, INNER_WIDTH), step_size_logits.reshape(block_list, BLOCK_LENGTH, HEAD_COUNT), extra_log_decay.reshape(block_list, BLOCK_LENGTH, HEAD_COUNT))
    unused_carry, mixer_rows = lax.scan(mixer_block, start, scan_results)
    mixer_rows = mixer_rows.reshape(TOKEN_COUNT, INNER_WIDTH)
    slice_width = INNER_WIDTH // N_TP
    mixed = jnp.zeros((TOKEN_COUNT, D), jnp.float32)
    for slice_index in range(N_TP):
        partial_value = jnp.dot(mixer_rows[:, slice_index * slice_width:(slice_index + 1) * slice_width], mixer_output_weight[slice_index * slice_width:(slice_index + 1) * slice_width], preferred_element_type=jnp.float32)
        rounded = lax.optimization_barrier(partial_value.astype(jnp.bfloat16))
        mixed = mixed + rounded.astype(jnp.float32)
    middle = layer_norm(ALPHA * residual.astype(jnp.float32) + mixed, first_norm_scale, first_norm_bias).astype(jnp.bfloat16)
    blocks_count = N_SP * N_TP
    rows_block = TOK_DEV // N_TP
    slot_ids = jax.vmap(partial_layout(CAP, EXPERTS))(routes.reshape(blocks_count, rows_block, TOPK))

    def fill_slots(block_rows, block_slots):
        owners = jnp.repeat(jnp.arange(rows_block, dtype=jnp.int32), TOPK)
        source = jnp.full((EXPERTS * CAP,), rows_block, jnp.int32).at[block_slots].set(owners)
        padded = jnp.concatenate([block_rows, jnp.zeros((1, D), jnp.bfloat16)], axis=0)
        return padded[source]
    buffers = jax.vmap(fill_slots)(middle.reshape(blocks_count, rows_block, D), slot_ids)
    buffers = buffers.reshape(blocks_count, EXPERTS, CAP, D)

    def one_expert(expert_index):
        rows_in = lax.dynamic_index_in_dim(buffers, expert_index, 1, keepdims=False).reshape(-1, D)
        weight_gate = lax.dynamic_index_in_dim(expert_gate_weight, expert_index, 0, keepdims=False)
        weight_up = lax.dynamic_index_in_dim(expert_up_weight, expert_index, 0, keepdims=False)
        weight_down = lax.dynamic_index_in_dim(expert_down_weight, expert_index, 0, keepdims=False)
        hidden = (jax.nn.silu(jnp.dot(rows_in, weight_gate, preferred_element_type=jnp.float32)) * jnp.dot(rows_in, weight_up, preferred_element_type=jnp.float32)).astype(jnp.bfloat16)
        return jnp.dot(hidden, weight_down.T, preferred_element_type=jnp.float32).astype(jnp.bfloat16)
    answers = lax.map(one_expert, jnp.arange(EXPERTS, dtype=jnp.int32))
    answers = answers.reshape(EXPERTS, blocks_count, CAP, D).transpose(1, 0, 2, 3).reshape(blocks_count, EXPERTS * CAP, D)

    def take_rows(block_answers, block_slots):
        return block_answers[block_slots]
    picked = jax.vmap(take_rows)(answers, slot_ids).astype(jnp.float32).reshape(TOKEN_COUNT, TOPK, D)
    ffn = lax.optimization_barrier(jnp.sum(picked * routing_weight[..., None], axis=1))
    return layer_norm(ALPHA * middle.astype(jnp.float32) + ffn, final_norm_scale, final_norm_bias).astype(jnp.bfloat16)
```

```python
import jax
import jax.numpy as jnp
from jax import lax
from jax.experimental import pallas as pl
from jax.experimental.pallas import tpu as pltpu
from jax.sharding import PartitionSpec as P


HEAD_DIM = 64
STATE_WIDTH = 128
BLOCK = 128
LANES = 128
SP = "sp"
SP_TP = ("sp", "tp")
EPS = 1e-05
ALPHA = 8.0**0.25
F32 = jnp.float32
BF16 = jnp.bfloat16

VMEM = pl.BlockSpec(memory_space=pltpu.VMEM)
SMEM = pl.BlockSpec(memory_space=pltpu.SMEM)
ANY = pl.BlockSpec(memory_space=pl.ANY)


def limit(mib):
    return pltpu.CompilerParams(vmem_limit_bytes=mib * 1024 * 1024)


def shape_of(shape, dtype):
    return jax.ShapeDtypeStruct(shape, dtype)


def near(shape, dtype):
    return pltpu.VMEM(shape, dtype)


def held(value):
    return pltpu.with_memory_space_constraint(value, pltpu.VMEM)


def far_off(*values):
    return [pltpu.with_memory_space_constraint(value, pltpu.HBM) for value in values]


def dot(a, b, dims=((1,), (0,))):
    return lax.dot_general(a, b, (dims, ((), ())), preferred_element_type=F32)


def silu(v):
    return v * (1.0 / (1.0 + jnp.exp(-v)))


def spread_heads(values, group, heads, width):
    total = values.shape[1]
    row = lax.broadcasted_iota(jnp.int32, (total, width), 0)
    col = lax.broadcasted_iota(jnp.int32, (total, width), 1)
    first = group * heads + col // HEAD_DIM
    pick = jnp.where(row == first, 1.0, 0.0).astype(BF16)
    high = values.astype(BF16)
    low = (values - high.astype(F32)).astype(BF16)
    return dot(high, pick) + dot(low, pick)


def fill_rows(rows_ref, tail_ref, raw_ref, cols, offset, length):
    rows_ref[0:8, :] = tail_ref[:, offset + cols.start : offset + cols.stop].astype(F32)
    rows_ref[8 : 8 + length, :] = raw_ref[:, cols].astype(F32)


def conv_cols(rows_ref, taps, length, margin):
    total = taps[0:1, :] * rows_ref[8 - margin : 8 - margin + length, :]
    for k in range(1, margin + 1):
        total = total + taps[k : k + 1, :] * rows_ref[8 - margin + k : 8 - margin + k + length, :]
    return silu(total)


def turned(ref):
    rows, length = ref.shape
    parts = []
    for i in range(0, length, BLOCK):
        tall = jnp.concatenate([ref[:, i : i + BLOCK], jnp.zeros((BLOCK - rows, BLOCK), F32)], axis=0)
        parts.append(tall.T[:, :rows])
    return jnp.concatenate(parts, axis=0)


def log_decays(logits_ref, extra_ref, bias_ref, rate_ref):
    raw = turned(logits_ref) + bias_ref[...]
    step = jnp.maximum(raw, 0.0) + jnp.log1p(jnp.exp(-jnp.abs(raw)))
    return step, -step * jnp.exp(rate_ref[...]) + turned(extra_ref)


def running_sum(block):
    t = lax.broadcasted_iota(jnp.int32, (BLOCK, BLOCK), 0)
    s = lax.broadcasted_iota(jnp.int32, (BLOCK, BLOCK), 1)
    lower = jnp.where(t >= s, 1.0, 0.0)
    return jnp.dot(lower, block, precision=lax.Precision.HIGHEST, preferred_element_type=F32)


def end_state_kernel(
    x_ref,
    b_ref,
    tail_ref,
    xf_ref,
    bf_ref,
    logits_ref,
    extra_ref,
    bias_ref,
    rate_ref,
    xc_ref,
    xdt_ref,
    bc_ref,
    running_ref,
    states_ref,
    message_ref,
    rows_ref,
):
    length, channels = x_ref.shape
    margin = xf_ref.shape[0] - 1
    groups = b_ref.shape[1] // STATE_WIDTH
    width = channels // groups
    heads = width // HEAD_DIM
    blocks = length // BLOCK
    step, decay = log_decays(logits_ref, extra_ref, bias_ref, rate_ref)
    sums = []
    for i in range(blocks):
        part = running_sum(decay[i * BLOCK : (i + 1) * BLOCK])
        running_ref[i * BLOCK : (i + 1) * BLOCK, :] = part
        sums.append(part)
    for c in range(0, groups * STATE_WIDTH, LANES):
        cols = slice(c, c + LANES)
        fill_rows(rows_ref, tail_ref, b_ref, cols, channels, length)
        bc_ref[:, cols] = conv_cols(rows_ref, bf_ref[:, cols].astype(F32), length, margin).astype(BF16)
    for c in range(0, channels, LANES):
        cols = slice(c, c + LANES)
        fill_rows(rows_ref, tail_ref, x_ref, cols, 0, length)
        xc_ref[:, cols] = conv_cols(rows_ref, xf_ref[:, cols].astype(F32), length, margin).astype(BF16)
    total = jnp.zeros((1, decay.shape[1]), F32)
    for i in range(blocks):
        total = total + sums[i][BLOCK - 1 : BLOCK]
    tiles = width // LANES
    for g in range(groups):
        state = None
        for i in range(blocks):
            rows = slice(i * BLOCK, (i + 1) * BLOCK)
            here = slice(g * width, (g + 1) * width)
            ending = sums[i][BLOCK - 1 : BLOCK]
            step_wide = spread_heads(step[rows], g, heads, width)
            left_wide = spread_heads(jnp.exp(ending - sums[i]), g, heads, width)
            scaled = xc_ref[rows, here].astype(F32) * step_wide
            xdt_ref[rows, here] = scaled.astype(BF16)
            keys = bc_ref[rows, g * STATE_WIDTH : (g + 1) * STATE_WIDTH].astype(F32).T.astype(BF16)
            added = dot(keys, (scaled * left_wide).astype(BF16))
            if state is None:
                state = added
            else:
                state = state * spread_heads(jnp.exp(ending), g, heads, width) + added
            if i + 1 < blocks:
                states_ref[i, g] = state
        high = total.astype(BF16)
        rest = total - high.astype(F32)
        low = rest.astype(BF16)
        least = (rest - low.astype(F32)).astype(BF16)
        parts = jnp.concatenate([high, low, least, jnp.zeros((5, total.shape[1]), BF16)], axis=0)
        logs = spread_heads(parts.astype(F32), g, heads, width).astype(BF16)
        for n in range(STATE_WIDTH // 16):
            for p in range(tiles):
                at = (g * (STATE_WIDTH // 16) + n) * tiles + p
                message_ref[at, 0:16, :] = state[n * 16 : (n + 1) * 16, p * LANES : (p + 1) * LANES].astype(BF16)
                message_ref[at, 16:24, :] = logs[:, p * LANES : (p + 1) * LANES]


def end_states(x, b, tail, xf, bf, logits, extra, bias, rate):
    length, channels = x.shape
    groups = b.shape[1] // STATE_WIDTH
    blocks = length // BLOCK
    width = channels // groups
    pieces = groups * STATE_WIDTH * width // (16 * LANES)
    return pl.pallas_call(
        end_state_kernel,
        out_shape=(
            pltpu.HBM((length, channels), BF16),
            pltpu.HBM((length, channels), BF16),
            pltpu.HBM(b.shape, BF16),
            pltpu.HBM((length, logits.shape[0]), F32),
            pltpu.HBM((blocks - 1, groups, STATE_WIDTH, width), F32),
            shape_of((pieces, 24, LANES), BF16),
        ),
        in_specs=[VMEM] * 9,
        out_specs=(VMEM,) * 6,
        scratch_shapes=[pltpu.VMEM((8 + length, LANES), F32)],
        compiler_params=limit(12),
        name="end_states",
    )(x, b, held(tail), xf, bf, logits, extra, bias, rate)


def chain_kernel(parts_ref, out_ref):
    peers = parts_ref.shape[0]

    def one(j, state):
        out_ref[j] = state.astype(BF16)
        logs = parts_ref[j, 16:24, :].astype(F32)
        factor = jnp.exp(logs[0:1] + logs[1:2] + logs[2:3])
        return state * factor + parts_ref[j, 0:16, :].astype(F32)

    lax.fori_loop(0, peers, one, jnp.zeros((16, LANES), F32), unroll=8)


def chain(parts):
    return pl.pallas_call(
        chain_kernel,
        out_shape=shape_of((parts.shape[0], 16, LANES), BF16),
        in_specs=[VMEM],
        out_specs=VMEM,
        compiler_params=limit(4),
        name="chain",
    )(held(parts))


def local_kernel(c_ref, tail_ref, cf_ref, bc_ref, xdt_ref, xc_ref, running_ref, direct_ref, cc_ref, y_ref, rows_ref):
    length, channels = xdt_ref.shape
    margin = cf_ref.shape[0] - 1
    groups = bc_ref.shape[1] // STATE_WIDTH
    width = channels // groups
    heads = width // HEAD_DIM
    offset = channels + groups * STATE_WIDTH
    for c in range(0, groups * STATE_WIDTH, LANES):
        cols = slice(c, c + LANES)
        fill_rows(rows_ref, tail_ref, c_ref, cols, offset, length)
        cc_ref[:, cols] = conv_cols(rows_ref, cf_ref[:, cols].astype(F32), length, margin).astype(BF16)
    t = lax.broadcasted_iota(jnp.int32, (BLOCK, BLOCK), 0)
    s = lax.broadcasted_iota(jnp.int32, (BLOCK, BLOCK), 1)
    causal = t >= s
    first_head = lax.broadcasted_iota(jnp.int32, (BLOCK, LANES), 1) < HEAD_DIM
    for i in range(length // BLOCK):
        rows = slice(i * BLOCK, (i + 1) * BLOCK)
        running = running_ref[rows, :]
        padded = jnp.concatenate([running, jnp.zeros((BLOCK, BLOCK - running.shape[1]), F32)], axis=1)
        across = padded.T
        for g in range(groups):
            wide = slice(g * STATE_WIDTH, (g + 1) * STATE_WIDTH)
            products = dot(cc_ref[rows, wide], bc_ref[rows, wide], ((1,), (1,)))
            products = jnp.where(causal, products, 0.0)
            for p in range(width // LANES):
                cols = slice(g * width + p * LANES, g * width + (p + 1) * LANES)
                pair = xdt_ref[rows, cols]
                total = direct_ref[:, cols] * xc_ref[rows, cols].astype(F32)
                for q in range(LANES // HEAD_DIM):
                    h = g * heads + p * (LANES // HEAD_DIM) + q
                    spread = running[:, h : h + 1] - across[h : h + 1, :]
                    weights = (products * jnp.exp(jnp.where(causal, spread, 0.0))).astype(BF16)
                    keep = first_head if q == 0 else ~first_head
                    total = total + dot(weights, jnp.where(keep, pair, jnp.zeros_like(pair)))
                y_ref[rows, cols] = total


def local_outputs(c, tail, cf, bc, xdt, xc, running, direct):
    length, channels = xdt.shape
    return pl.pallas_call(
        local_kernel,
        out_shape=(pltpu.HBM(c.shape, BF16), pltpu.HBM((length, channels), F32)),
        in_specs=[VMEM] * 8,
        out_specs=(VMEM, VMEM),
        scratch_shapes=[pltpu.VMEM((8 + length, LANES), F32)],
        compiler_params=limit(12),
        name="local_outputs",
    )(c, tail, cf, bc, xdt, xc, running, direct)


def project_kernel(y_ref, cc_ref, states_ref, incoming_ref, running_ref, gate_ref, scale_ref, w_hbm, out_ref, w_ref, rows_ref, sem):
    copy = pltpu.make_async_copy(w_hbm, w_ref, sem)
    copy.start()
    length, channels = y_ref.shape
    groups = cc_ref.shape[1] // STATE_WIDTH
    width = channels // groups
    heads = width // HEAD_DIM
    tiles = width // LANES
    for g in range(groups):
        here = slice(g * width, (g + 1) * width)
        wide = slice(g * STATE_WIDTH, (g + 1) * STATE_WIDTH)
        lines = []
        for n in range(STATE_WIDTH // 16):
            at = (g * (STATE_WIDTH // 16) + n) * tiles
            lines.append(jnp.concatenate([incoming_ref[at + p] for p in range(tiles)], axis=1))
        incoming = jnp.concatenate(lines, axis=0).astype(F32)
        started = jnp.zeros((1, running_ref.shape[1]), F32)
        for i in range(length // BLOCK):
            rows = slice(i * BLOCK, (i + 1) * BLOCK)
            running = running_ref[rows, :]
            if i == 0:
                state = incoming
            else:
                state = states_ref[i - 1, g] + incoming * spread_heads(jnp.exp(started), g, heads, width)
            started = started + running[BLOCK - 1 : BLOCK]
            read = dot(cc_ref[rows, wide], state.astype(BF16)) * spread_heads(jnp.exp(running), g, heads, width)
            gated = (y_ref[rows, here] + read) * silu(gate_ref[rows, here].astype(F32))
            power = jnp.mean(gated * gated, axis=1, keepdims=True)
            normed = gated * lax.rsqrt(power + EPS) * scale_ref[:, here].astype(F32)
            rows_ref[rows, here] = normed.astype(BF16)
    copy.wait()
    out_ref[...] = dot(rows_ref[...], w_ref[...]).astype(BF16)


def projected(y, cc, states, incoming, running, gate, scale, w):
    length, channels = y.shape
    return pl.pallas_call(
        project_kernel,
        out_shape=shape_of((length, w.shape[1]), BF16),
        in_specs=[VMEM] * 7 + [ANY],
        out_specs=VMEM,
        scratch_shapes=[
            pltpu.VMEM(w.shape, BF16),
            pltpu.VMEM((length, channels), BF16),
            pltpu.SemaphoreType.DMA,
        ],
        compiler_params=limit(20),
        name="projected",
    )(y, cc, states, held(incoming), running, gate, scale, *far_off(w))


def slots_kernel(capacity, routes_ref, slots_ref, count_ref):
    def clear(e, carry):
        count_ref[e] = 0
        return carry

    lax.fori_loop(0, count_ref.shape[0], clear, 0, unroll=8)

    def one(r, carry):
        for k in range(routes_ref.shape[0]):
            e = routes_ref[k, r]
            used = count_ref[e]
            count_ref[e] = used + 1
            slots_ref[k, r] = e * capacity + used
        return carry

    lax.fori_loop(0, routes_ref.shape[1], one, 0, unroll=4)


def slot_layout(routes, capacity, experts):
    return pl.pallas_call(
        lambda *refs: slots_kernel(capacity, *refs),
        out_shape=shape_of(routes.shape, jnp.int32),
        in_specs=[SMEM],
        out_specs=SMEM,
        scratch_shapes=[pltpu.SMEM((experts,), jnp.int32)],
        compiler_params=limit(1),
        name="slot_layout",
    )(routes)


def layer_norm(values, gain_row, bias_row):
    mean_value = jnp.mean(values, axis=-1, keepdims=True)
    centred = values - mean_value
    spread = jnp.mean(centred * centred, axis=-1, keepdims=True)
    return centred * lax.rsqrt(spread + EPS) * gain_row + bias_row


def middle_kernel(top_count, parts_ref, residual_ref, gain_ref, bias_ref, slots_ref, middle_ref, out_ref, blocks_ref):
    rows_here, width = residual_ref.shape
    chunks = width // LANES
    for r in range(0, rows_here, 16):
        rows = slice(r, r + 16)
        mixed = parts_ref[0, rows, :].astype(F32)
        for k in range(1, parts_ref.shape[0]):
            mixed = mixed + parts_ref[k, rows, :].astype(F32)
        values = layer_norm(ALPHA * residual_ref[rows, :].astype(F32) + mixed, gain_ref[...], bias_ref[...])
        for c in range(chunks):
            blocks_ref[pl.ds(r * chunks + c, 16, stride=chunks), :] = values[:, c * LANES : (c + 1) * LANES]

    def one(r, carry):
        at = pl.multiple_of(r * chunks, 16)
        block = blocks_ref[pl.ds(at, chunks), :].astype(BF16)
        middle_ref[r] = block
        for k in range(top_count):
            out_ref[slots_ref[k, r]] = block
        return carry

    lax.fori_loop(0, rows_here, one, 0, unroll=4)


def middle_rows(parts, residual, gain, bias, slots, top_count, slot_total):
    rows_here, width = residual.shape
    chunks = width // LANES
    return pl.pallas_call(
        lambda *refs: middle_kernel(top_count, *refs),
        out_shape=(
            shape_of((rows_here, chunks, LANES), BF16),
            shape_of((slot_total, chunks, LANES), BF16),
        ),
        in_specs=[VMEM] * 4 + [SMEM],
        out_specs=(VMEM, VMEM),
        scratch_shapes=[pltpu.VMEM((rows_here * chunks, LANES), F32)],
        compiler_params=limit(8),
        name="middle_rows",
    )(held(parts), residual, gain, bias, slots)


def expert_kernel(arrived_ref, *refs):
    pieces = refs[:-6]
    out_ref, blocks_ref, x_ref, hidden_ref, buffer_ref, sem = refs[-6:]
    slots, chunks, _ = arrived_ref.shape
    width = chunks * LANES
    quarters, _, units = buffer_ref.shape
    copies = []
    for n, source in enumerate(pieces):
        size = source.shape[0]
        own = n < 3
        quarter = 0 if own else 1 + (n - 3) // 2
        start = n * width if own else (n - 3) % 2 * size
        copies.append((quarter, pltpu.make_async_copy(source, buffer_ref.at[quarter, pl.ds(start, size)], sem.at[n])))
    for _, copy in copies:
        copy.start()
    for s in range(0, slots, 16):
        blocks_ref[s * chunks : (s + 16) * chunks, :] = arrived_ref[s : s + 16].reshape(16 * chunks, LANES).astype(F32)
    for c in range(chunks):
        x_ref[:, c * LANES : (c + 1) * LANES] = blocks_ref[pl.ds(c, slots, stride=chunks), :].astype(BF16)
    for q in range(quarters):
        for quarter, copy in copies:
            if quarter == q:
                copy.wait()
        gate = dot(x_ref[...], buffer_ref[q, :width, :])
        up = dot(x_ref[...], buffer_ref[q, width : 2 * width, :])
        hidden_ref[:, q * units : (q + 1) * units] = (silu(gate) * up).astype(BF16)
    step = 512
    for n in range(0, width, step):
        total = None
        for q in range(quarters):
            down = buffer_ref[q, 2 * width + n : 2 * width + n + step, :]
            part = dot(hidden_ref[:, q * units : (q + 1) * units], down, ((1,), (1,)))
            total = part if total is None else total + part
        for c in range(step // LANES):
            blocks_ref[pl.ds(n // LANES + c, slots, stride=chunks), :] = total[:, c * LANES : (c + 1) * LANES]
    for s in range(0, slots, 16):
        out_ref[s : s + 16] = blocks_ref[s * chunks : (s + 16) * chunks, :].astype(BF16).reshape(16, chunks, LANES)


def expert_answers(arrived, own, packs):
    slots, chunks, _ = arrived.shape
    width = chunks * LANES
    units = own[0].shape[1]
    pieces = [*own, *packs]
    return pl.pallas_call(
        expert_kernel,
        out_shape=shape_of(arrived.shape, BF16),
        in_specs=[VMEM] + [ANY] * len(pieces),
        out_specs=VMEM,
        scratch_shapes=[
            pltpu.VMEM((slots * chunks, LANES), F32),
            pltpu.VMEM((slots, width), BF16),
            pltpu.VMEM((slots, 4 * units), BF16),
            pltpu.VMEM((4, 3 * width, units), BF16),
            pltpu.SemaphoreType.DMA((len(pieces),)),
        ],
        compiler_params=limit(36),
        name="expert_answers",
    )(held(arrived), *far_off(*pieces))


def pack_kernel(gate_ref, up_ref, down_ref, first_ref, second_ref, stage_ref, into, out):
    width = gate_ref.shape[0]
    half = width // 2
    sources = (
        gate_ref.at[pl.ds(0, half)],
        gate_ref.at[pl.ds(half, half)],
        up_ref.at[pl.ds(0, half)],
        up_ref.at[pl.ds(half, half)],
        down_ref.at[pl.ds(0, half)],
        down_ref.at[pl.ds(half, half)],
    )
    loads = [pltpu.make_async_copy(source, stage_ref.at[n], into.at[n]) for n, source in enumerate(sources)]
    stores = []
    for n in range(len(sources)):
        target = first_ref if n < 3 else second_ref
        stores.append(pltpu.make_async_copy(stage_ref.at[n], target.at[pl.ds(n % 3 * half, half)], out.at[n]))
    for load in loads:
        load.start()
    for load, store in zip(loads, stores):
        load.wait()
        store.start()
    for store in stores:
        store.wait()


def packed(gate, up, down):
    width, units = gate.shape
    both = pltpu.HBM((width * 3 // 2, units), BF16)
    return pl.pallas_call(
        pack_kernel,
        out_shape=(both, both),
        in_specs=[ANY] * 3,
        out_specs=(ANY, ANY),
        scratch_shapes=[
            pltpu.VMEM((6, width // 2, units), BF16),
            pltpu.SemaphoreType.DMA((6,)),
            pltpu.SemaphoreType.DMA((6,)),
        ],
        compiler_params=limit(8),
        name="packed",
    )(*far_off(gate, up, down))


def tail_kernel(x_ref, b_ref, c_ref, out_ref, sem):
    rows = out_ref.shape[0]
    copies = []
    start = 0
    for n, ref in enumerate((x_ref, b_ref, c_ref)):
        length, width = ref.shape
        source = ref.at[pl.ds(length - rows, rows)]
        copies.append(pltpu.make_async_copy(source, out_ref.at[:, pl.ds(start, width)], sem.at[n]))
        start += width
    for copy in copies:
        copy.start()
    for copy in copies:
        copy.wait()


def last_rows(x, b, c, rows):
    return pl.pallas_call(
        tail_kernel,
        out_shape=near((rows, x.shape[1] + b.shape[1] + c.shape[1]), BF16),
        in_specs=[ANY] * 3,
        out_specs=VMEM,
        scratch_shapes=[pltpu.SemaphoreType.DMA((3,))],
        compiler_params=limit(1),
        name="last_rows",
    )(*far_off(x, b, c))


def final_kernel(top_count, returned_ref, middle_ref, slots_ref, weights_ref, gain_ref, bias_ref, out_ref, blocks_ref):
    rows_here, chunks, _ = middle_ref.shape

    def one(r, carry):
        total = returned_ref[slots_ref[0, r]].astype(F32) * weights_ref[0, r]
        for k in range(1, top_count):
            total = total + returned_ref[slots_ref[k, r]].astype(F32) * weights_ref[k, r]
        start = pl.multiple_of(r * chunks, 16)
        blocks_ref[pl.ds(start, chunks), :] = ALPHA * middle_ref[r].astype(F32) + total
        return carry

    lax.fori_loop(0, rows_here, one, 0, unroll=4)
    for r in range(0, rows_here, 16):
        values = jnp.concatenate(
            [blocks_ref[pl.ds(r * chunks + c, 16, stride=chunks), :] for c in range(chunks)], axis=1
        )
        out_ref[r : r + 16, :] = layer_norm(values, gain_ref[...], bias_ref[...]).astype(BF16)


def final_rows(returned, middle, slots, weights, gain, bias, top_count):
    rows_here, chunks, _ = middle.shape
    return pl.pallas_call(
        lambda *refs: final_kernel(top_count, *refs),
        out_shape=shape_of((rows_here, chunks * LANES), BF16),
        in_specs=[VMEM, VMEM, SMEM, SMEM, VMEM, VMEM],
        out_specs=VMEM,
        scratch_shapes=[pltpu.VMEM((rows_here * chunks, LANES), F32)],
        compiler_params=limit(8),
        name="final_rows",
    )(held(returned), middle, slots, weights, gain, bias)


def turned_by(value, distance):
    peers = lax.axis_size("tp")
    return lax.ppermute(value, "tp", [(i, (i + distance) % peers) for i in range(peers)])


def exchanged(value, axis):
    return lax.all_to_all(value, axis, split_axis=0, concat_axis=0, tiled=True)


def shards(
    head_input_values,
    group_input_vectors,
    group_readout_vectors,
    output_gate_values,
    step_size_logits,
    extra_log_decay,
    head_input_filter,
    input_vector_filter,
    readout_vector_filter,
    step_size_bias,
    head_rate_logarithm,
    direct_path_weight,
    group_norm_scale,
    mixer_output_weight,
    residual,
    first_norm_scale,
    first_norm_bias,
    routes,
    routing_weight,
    expert_gate_weight,
    expert_up_weight,
    expert_down_weight,
    final_norm_scale,
    final_norm_bias,
):
    devices = lax.axis_size(SP)
    experts = expert_gate_weight.shape[0] * devices
    rows_here, top_count = routes.shape
    width = residual.shape[1]
    capacity = 5

    own = (expert_gate_weight[0], expert_up_weight[0], expert_down_weight[0])
    ending = last_rows(head_input_values, group_input_vectors, group_readout_vectors, 8)
    tail = lax.ppermute(ending, SP, [(i, i + 1) for i in range(devices - 1)])
    first, second = packed(*own)
    first_behind = turned_by(first, 1)
    first_ahead = turned_by(first, -1)
    second_behind = turned_by(second, 1)
    second_ahead = turned_by(second, -1)
    xc, xdt, bc, running, states, message = end_states(
        head_input_values,
        group_input_vectors,
        tail,
        head_input_filter,
        input_vector_filter,
        step_size_logits.T,
        extra_log_decay.T,
        step_size_bias[None],
        head_rate_logarithm[None],
    )
    met = exchanged(message, SP)
    slots = slot_layout(routes.T, capacity, experts)
    direct = jnp.repeat(direct_path_weight, HEAD_DIM)[None]
    cc, y = local_outputs(group_readout_vectors, tail, readout_vector_filter, bc, xdt, xc, running, direct)
    incoming = exchanged(chain(met), SP)
    sums = projected(
        y, cc, states, incoming, running, output_gate_values, group_norm_scale[None], mixer_output_weight
    )
    peers = lax.axis_size("tp")
    parts = exchanged(sums.reshape(peers, rows_here, width), "tp")
    first_behind, second_ahead, parts = lax.optimization_barrier((first_behind, second_ahead, parts))
    first_far = turned_by(first_behind, 1)
    second_far = turned_by(second_ahead, -1)
    middle, outgoing = middle_rows(
        parts, residual, first_norm_scale[None], first_norm_bias[None], slots, top_count, experts * capacity
    )
    chunks = width // LANES
    arrived = exchanged(outgoing.reshape(experts, capacity * chunks, LANES), SP)
    answers = expert_answers(
        arrived.reshape(experts * capacity, chunks, LANES),
        own,
        (first_behind, second_behind, first_ahead, second_ahead, first_far, second_far),
    )
    returned = exchanged(answers.reshape(experts, capacity * chunks, LANES), SP)
    return final_rows(
        returned.reshape(experts * capacity, chunks, LANES),
        middle,
        slots,
        routing_weight.T,
        final_norm_scale[None],
        final_norm_bias[None],
        top_count,
    )


def solution(mesh):
    placed = (
        P(SP, "tp"),
        P(SP, "tp"),
        P(SP, "tp"),
        P(SP, "tp"),
        P(SP, "tp"),
        P(SP, "tp"),
        P(None, "tp"),
        P(None, "tp"),
        P(None, "tp"),
        P("tp"),
        P("tp"),
        P("tp"),
        P("tp"),
        P("tp", None),
        P(SP_TP, None),
        P(),
        P(),
        P(SP_TP, None),
        P(SP_TP, None),
        P(SP, None, "tp"),
        P(SP, None, "tp"),
        P(SP, None, "tp"),
        P(),
        P(),
    )
    return jax.shard_map(shards, mesh=mesh, in_specs=placed, out_specs=P(SP_TP, None), check_vma=False)
```

```python
import jax
import jax.numpy as jnp
from jax import lax
from jax.experimental import pallas as pl
from jax.experimental.pallas import tpu as pltpu
from jax.sharding import PartitionSpec as P


HEAD_DIM = 64
STATE_WIDTH = 128
BLOCK = 128
LANES = 128
PITCH = 20
SP = "sp"
SP_TP = ("sp", "tp")
EPS = 1e-05
ALPHA = 8.0**0.25
F32 = jnp.float32
BF16 = jnp.bfloat16

VMEM = pl.BlockSpec(memory_space=pltpu.VMEM)
SMEM = pl.BlockSpec(memory_space=pltpu.SMEM)
ANY = pl.BlockSpec(memory_space=pl.ANY)


def limit(mib):
    return pltpu.CompilerParams(vmem_limit_bytes=mib * 1024 * 1024)


def shape_of(shape, dtype):
    return jax.ShapeDtypeStruct(shape, dtype)


def near(shape, dtype):
    return pltpu.VMEM(shape, dtype)


def held(value):
    return pltpu.with_memory_space_constraint(value, pltpu.VMEM)


def far_off(*values):
    return [pltpu.with_memory_space_constraint(value, pltpu.HBM) for value in values]


def dot(a, b, dims=((1,), (0,))):
    return lax.dot_general(a, b, (dims, ((), ())), preferred_element_type=F32)


def silu(v):
    return 0.5 * v * (1.0 + jnp.tanh(0.5 * v))


def spread_heads(values, group, heads, width):
    total = values.shape[1]
    row = lax.broadcasted_iota(jnp.int32, (total, width), 0)
    col = lax.broadcasted_iota(jnp.int32, (total, width), 1)
    first = group * heads + col // HEAD_DIM
    pick = jnp.where(row == first, 1.0, 0.0).astype(BF16)
    high = values.astype(BF16)
    low = (values - high.astype(F32)).astype(BF16)
    return dot(high, pick) + dot(low, pick)


def fill_rows(rows_ref, tail_ref, raw_ref, cols, offset, length):
    rows_ref[0:8, :] = tail_ref[:, offset + cols.start : offset + cols.stop].astype(F32)
    rows_ref[8 : 8 + length, :] = raw_ref[:, cols].astype(F32)


def conv_cols(rows_ref, taps, length, margin):
    total = taps[0:1, :] * rows_ref[8 - margin : 8 - margin + length, :]
    for k in range(1, margin + 1):
        total = total + taps[k : k + 1, :] * rows_ref[8 - margin + k : 8 - margin + k + length, :]
    return silu(total)


def turned(ref):
    rows, length = ref.shape
    parts = []
    for i in range(0, length, BLOCK):
        tall = jnp.concatenate([ref[:, i : i + BLOCK], jnp.zeros((BLOCK - rows, BLOCK), F32)], axis=0)
        parts.append(tall.T[:, :rows])
    return jnp.concatenate(parts, axis=0)


def log_decays(logits_ref, extra_ref, bias_ref, rate_ref):
    raw = turned(logits_ref) + bias_ref[...]
    step = jnp.maximum(raw, 0.0) + jnp.log1p(jnp.exp(-jnp.abs(raw)))
    return step, -step * jnp.exp(rate_ref[...]) + turned(extra_ref)


def running_sum(block):
    t = lax.broadcasted_iota(jnp.int32, (BLOCK, BLOCK), 0)
    s = lax.broadcasted_iota(jnp.int32, (BLOCK, BLOCK), 1)
    lower = jnp.where(t >= s, 1.0, 0.0)
    return jnp.dot(lower, block, precision=lax.Precision.HIGHEST, preferred_element_type=F32)


def end_state_kernel(
    x_ref,
    b_ref,
    tail_ref,
    xf_ref,
    bf_ref,
    logits_ref,
    extra_ref,
    bias_ref,
    rate_ref,
    xc_ref,
    xdt_ref,
    bc_ref,
    running_ref,
    states_ref,
    message_ref,
    rows_ref,
):
    length, channels = x_ref.shape
    margin = xf_ref.shape[0] - 1
    groups = b_ref.shape[1] // STATE_WIDTH
    width = channels // groups
    heads = width // HEAD_DIM
    blocks = length // BLOCK
    step, decay = log_decays(logits_ref, extra_ref, bias_ref, rate_ref)
    sums = []
    for i in range(blocks):
        part = running_sum(decay[i * BLOCK : (i + 1) * BLOCK])
        running_ref[i * BLOCK : (i + 1) * BLOCK, :] = part
        sums.append(part)
    for c in range(0, groups * STATE_WIDTH, LANES):
        cols = slice(c, c + LANES)
        fill_rows(rows_ref, tail_ref, b_ref, cols, channels, length)
        bc_ref[:, cols] = conv_cols(rows_ref, bf_ref[:, cols].astype(F32), length, margin).astype(BF16)
    for c in range(0, channels, LANES):
        cols = slice(c, c + LANES)
        fill_rows(rows_ref, tail_ref, x_ref, cols, 0, length)
        xc_ref[:, cols] = conv_cols(rows_ref, xf_ref[:, cols].astype(F32), length, margin).astype(BF16)
    total = jnp.zeros((1, decay.shape[1]), F32)
    for i in range(blocks):
        total = total + sums[i][BLOCK - 1 : BLOCK]
    tiles = width // LANES
    for g in range(groups):
        state = None
        for i in range(blocks):
            rows = slice(i * BLOCK, (i + 1) * BLOCK)
            here = slice(g * width, (g + 1) * width)
            ending = sums[i][BLOCK - 1 : BLOCK]
            step_wide = spread_heads(step[rows], g, heads, width)
            left_wide = spread_heads(jnp.exp(ending - sums[i]), g, heads, width)
            scaled = xc_ref[rows, here].astype(F32) * step_wide
            xdt_ref[rows, here] = scaled.astype(BF16)
            keys = bc_ref[rows, g * STATE_WIDTH : (g + 1) * STATE_WIDTH].astype(F32).T.astype(BF16)
            added = dot(keys, (scaled * left_wide).astype(BF16))
            if state is None:
                state = added
            else:
                state = state * spread_heads(jnp.exp(ending), g, heads, width) + added
            if i + 1 < blocks:
                states_ref[i, g] = state
        high = total.astype(BF16)
        rest = total - high.astype(F32)
        low = rest.astype(BF16)
        least = (rest - low.astype(F32)).astype(BF16)
        parts = jnp.concatenate([high, low, least, jnp.zeros((5, total.shape[1]), BF16)], axis=0)
        logs = spread_heads(parts.astype(F32), g, heads, width).astype(BF16)
        for n in range(STATE_WIDTH // 16):
            for p in range(tiles):
                at = (g * (STATE_WIDTH // 16) + n) * tiles + p
                message_ref[at, 0:16, :] = state[n * 16 : (n + 1) * 16, p * LANES : (p + 1) * LANES].astype(BF16)
                message_ref[at, 16:24, :] = logs[:, p * LANES : (p + 1) * LANES]


def end_states(tail, x, b, xf, bf, logits, extra, bias, rate):
    length, channels = x.shape
    groups = b.shape[1] // STATE_WIDTH
    blocks = length // BLOCK
    width = channels // groups
    pieces = groups * STATE_WIDTH * width // (16 * LANES)
    return pl.pallas_call(
        end_state_kernel,
        out_shape=(
            pltpu.HBM((length, channels), BF16),
            pltpu.HBM((length, channels), BF16),
            pltpu.HBM(b.shape, BF16),
            pltpu.HBM((length, logits.shape[0]), F32),
            pltpu.HBM((blocks - 1, groups, STATE_WIDTH, width), F32),
            shape_of((pieces, 24, LANES), BF16),
        ),
        in_specs=[VMEM] * 9,
        out_specs=(VMEM,) * 6,
        scratch_shapes=[pltpu.VMEM((8 + length, LANES), F32)],
        compiler_params=limit(12),
        name="end_states",
    )(*map(held, (x, b, tail, xf, bf, logits, extra, bias, rate)))


def chain_kernel(parts_ref, out_ref):
    peers = parts_ref.shape[0]

    def one(j, state):
        out_ref[j] = state.astype(BF16)
        logs = parts_ref[j, 16:24, :].astype(F32)
        factor = jnp.exp(logs[0:1] + logs[1:2] + logs[2:3])
        return state * factor + parts_ref[j, 0:16, :].astype(F32)

    lax.fori_loop(0, peers, one, jnp.zeros((16, LANES), F32), unroll=8)


def chain(parts):
    return pl.pallas_call(
        chain_kernel,
        out_shape=shape_of((parts.shape[0], 16, LANES), BF16),
        in_specs=[VMEM],
        out_specs=VMEM,
        compiler_params=limit(4),
        name="chain",
    )(held(parts))


def local_kernel(
    c_ref,
    tail_ref,
    cf_ref,
    bc_ref,
    xdt_ref,
    xc_ref,
    running_ref,
    states_ref,
    direct_ref,
    gate_ref,
    cc_ref,
    fixed_ref,
    factor_ref,
    rows_ref,
):
    length, channels = xdt_ref.shape
    margin = cf_ref.shape[0] - 1
    groups = bc_ref.shape[1] // STATE_WIDTH
    width = channels // groups
    heads = width // HEAD_DIM
    offset = channels + groups * STATE_WIDTH
    for c in range(0, groups * STATE_WIDTH, LANES):
        cols = slice(c, c + LANES)
        fill_rows(rows_ref, tail_ref, c_ref, cols, offset, length)
        cc_ref[:, cols] = conv_cols(rows_ref, cf_ref[:, cols].astype(F32), length, margin).astype(BF16)
    t = lax.broadcasted_iota(jnp.int32, (BLOCK, BLOCK), 0)
    s = lax.broadcasted_iota(jnp.int32, (BLOCK, BLOCK), 1)
    causal = t >= s
    first_head = lax.broadcasted_iota(jnp.int32, (BLOCK, LANES), 1) < HEAD_DIM
    started = jnp.zeros((1, running_ref.shape[1]), F32)
    for i in range(length // BLOCK):
        rows = slice(i * BLOCK, (i + 1) * BLOCK)
        running = running_ref[rows, :]
        padded = jnp.concatenate([running, jnp.zeros((BLOCK, BLOCK - running.shape[1]), F32)], axis=1)
        across = padded.T
        since_block = jnp.exp(running)
        since_start = jnp.exp(running + started)
        started = started + running[BLOCK - 1 : BLOCK]
        for g in range(groups):
            here = slice(g * width, (g + 1) * width)
            wide = slice(g * STATE_WIDTH, (g + 1) * STATE_WIDTH)
            products = dot(cc_ref[rows, wide], bc_ref[rows, wide], ((1,), (1,)))
            products = jnp.where(causal, products, 0.0)
            gate = silu(gate_ref[rows, here].astype(F32))
            factor_ref[rows, here] = (spread_heads(since_start, g, heads, width) * gate).astype(BF16)
            carried = None
            if i > 0:
                read = dot(cc_ref[rows, wide], states_ref[i - 1, g].astype(BF16))
                carried = read * spread_heads(since_block, g, heads, width)
            for p in range(width // LANES):
                part = slice(p * LANES, (p + 1) * LANES)
                cols = slice(g * width + p * LANES, g * width + (p + 1) * LANES)
                pair = xdt_ref[rows, cols]
                total = direct_ref[:, cols] * xc_ref[rows, cols].astype(F32)
                if carried is not None:
                    total = total + carried[:, part]
                for q in range(LANES // HEAD_DIM):
                    h = g * heads + p * (LANES // HEAD_DIM) + q
                    spread = running[:, h : h + 1] - across[h : h + 1, :]
                    weights = (products * jnp.exp(jnp.where(causal, spread, 0.0))).astype(BF16)
                    keep = first_head if q == 0 else ~first_head
                    total = total + dot(weights, jnp.where(keep, pair, jnp.zeros_like(pair)))
                fixed_ref[rows, cols] = (total * gate[:, part]).astype(BF16)


def local_outputs(c, tail, cf, bc, xdt, xc, running, states, direct, gate):
    length, channels = xdt.shape
    return pl.pallas_call(
        local_kernel,
        out_shape=(
            near(c.shape, BF16),
            near((length, channels), BF16),
            near((length, channels), BF16),
        ),
        in_specs=[VMEM] * 10,
        out_specs=(VMEM,) * 3,
        scratch_shapes=[pltpu.VMEM((8 + length, LANES), F32)],
        compiler_params=limit(14),
        name="local_outputs",
    )(c, tail, cf, bc, xdt, xc, running, states, direct, gate)


def project_kernel(fixed_ref, factor_ref, cc_ref, incoming_ref, scale_ref, w_hbm, out_ref, w_ref, rows_ref, sem):
    copy = pltpu.make_async_copy(w_hbm, w_ref, sem)
    copy.start()
    length, channels = fixed_ref.shape
    groups = cc_ref.shape[1] // STATE_WIDTH
    width = channels // groups
    tiles = width // LANES
    for g in range(groups):
        here = slice(g * width, (g + 1) * width)
        wide = slice(g * STATE_WIDTH, (g + 1) * STATE_WIDTH)
        lines = []
        for n in range(STATE_WIDTH // 16):
            at = (g * (STATE_WIDTH // 16) + n) * tiles
            lines.append(jnp.concatenate([incoming_ref[at + p] for p in range(tiles)], axis=1))
        incoming = jnp.concatenate(lines, axis=0)
        for i in range(length // BLOCK):
            rows = slice(i * BLOCK, (i + 1) * BLOCK)
            read = dot(cc_ref[rows, wide], incoming)
            gated = fixed_ref[rows, here].astype(F32) + read * factor_ref[rows, here].astype(F32)
            power = jnp.mean(gated * gated, axis=1, keepdims=True)
            normed = gated * lax.rsqrt(power + EPS) * scale_ref[:, here].astype(F32)
            rows_ref[rows, here] = normed.astype(BF16)
    copy.wait()
    out_ref[...] = dot(rows_ref[...], w_ref[...]).astype(BF16)


def projected(fixed, factor, cc, incoming, scale, w):
    length, channels = fixed.shape
    return pl.pallas_call(
        project_kernel,
        out_shape=near((length, w.shape[1]), BF16),
        in_specs=[VMEM] * 5 + [ANY],
        out_specs=VMEM,
        scratch_shapes=[
            pltpu.VMEM(w.shape, BF16),
            pltpu.VMEM((length, channels), BF16),
            pltpu.SemaphoreType.DMA,
        ],
        compiler_params=limit(20),
        name="projected",
    )(held(fixed), held(factor), held(cc), held(incoming), scale, *far_off(w))


def slots_kernel(capacity, routes_ref, slots_ref, count_ref):
    def clear(e, carry):
        count_ref[e] = 0
        return carry

    lax.fori_loop(0, count_ref.shape[0], clear, 0, unroll=8)

    def one(r, carry):
        for k in range(routes_ref.shape[0]):
            e = routes_ref[k, r]
            used = count_ref[e]
            count_ref[e] = used + 1
            slots_ref[k, r] = e * capacity + used
        return carry

    lax.fori_loop(0, routes_ref.shape[1], one, 0, unroll=4)


def slot_layout(routes, capacity, experts):
    return pl.pallas_call(
        lambda *refs: slots_kernel(capacity, *refs),
        out_shape=shape_of(routes.shape, jnp.int32),
        in_specs=[SMEM],
        out_specs=SMEM,
        scratch_shapes=[pltpu.SMEM((experts,), jnp.int32)],
        compiler_params=limit(1),
        name="slot_layout",
    )(routes)


def layer_norm(values, gain_row, bias_row):
    mean_value = jnp.mean(values, axis=-1, keepdims=True)
    centred = values - mean_value
    spread = jnp.mean(centred * centred, axis=-1, keepdims=True)
    return centred * lax.rsqrt(spread + EPS) * gain_row + bias_row


def middle_kernel(top_count, parts_ref, residual_ref, gain_ref, bias_ref, slots_ref, middle_ref, out_ref, blocks_ref):
    rows_here, width = residual_ref.shape
    chunks = width // LANES
    for r in range(0, rows_here, 16):
        rows = slice(r, r + 16)
        mixed = parts_ref[0, rows, :].astype(F32)
        for k in range(1, parts_ref.shape[0]):
            mixed = mixed + parts_ref[k, rows, :].astype(F32)
        values = layer_norm(ALPHA * residual_ref[rows, :].astype(F32) + mixed, gain_ref[...], bias_ref[...])
        for c in range(chunks):
            blocks_ref[pl.ds(r * chunks + c, 16, stride=chunks), :] = values[:, c * LANES : (c + 1) * LANES]

    def one(r, carry):
        at = pl.multiple_of(r * chunks, 16)
        block = blocks_ref[pl.ds(at, chunks), :].astype(BF16)
        middle_ref[r] = block
        for k in range(top_count):
            out_ref[slots_ref[k, r]] = block
        return carry

    lax.fori_loop(0, rows_here, one, 0, unroll=4)


def middle_rows(parts, residual, gain, bias, slots, top_count, slot_total):
    rows_here, width = residual.shape
    chunks = width // LANES
    return pl.pallas_call(
        lambda *refs: middle_kernel(top_count, *refs),
        out_shape=(
            shape_of((rows_here, chunks, LANES), BF16),
            shape_of((slot_total, chunks, LANES), BF16),
        ),
        in_specs=[VMEM] * 4 + [SMEM],
        out_specs=(VMEM, VMEM),
        scratch_shapes=[pltpu.VMEM((rows_here * chunks, LANES), F32)],
        compiler_params=limit(8),
        name="middle_rows",
    )(held(parts), residual, gain, bias, slots)


def expert_kernel(places, arrived_ref, *refs):
    pieces = refs[:-6]
    out_ref, blocks_ref, x_ref, hidden_ref, buffer_ref, sem = refs[-6:]
    slots, chunks, _ = arrived_ref.shape
    width = chunks * LANES
    quarters, _, units = buffer_ref.shape
    copies = []
    for n, (which, at, size, quarter, to) in enumerate(places):
        source = pieces[which].at[pl.ds(at, size)]
        copies.append((quarter, pltpu.make_async_copy(source, buffer_ref.at[quarter, pl.ds(to, size)], sem.at[n])))
    for _, copy in copies:
        copy.start()
    for s in range(0, slots, 16):
        for r in range(s, s + 16):
            blocks_ref[r * PITCH : r * PITCH + chunks, :] = arrived_ref[r].astype(F32)
    for c in range(chunks):
        x_ref[:, c * LANES : (c + 1) * LANES] = blocks_ref[pl.ds(c, slots, stride=PITCH), :].astype(BF16)
    for q in range(quarters):
        for quarter, copy in copies:
            if quarter == q:
                copy.wait()
        gate = dot(x_ref[...], buffer_ref[q, :width, :])
        up = dot(x_ref[...], buffer_ref[q, width : 2 * width, :])
        hidden_ref[:, q * units : (q + 1) * units] = (silu(gate) * up).astype(BF16)
    step = 512
    for n in range(0, width, step):
        total = None
        for q in range(quarters):
            down = buffer_ref[q, 2 * width + n : 2 * width + n + step, :]
            part = dot(hidden_ref[:, q * units : (q + 1) * units], down, ((1,), (1,)))
            total = part if total is None else total + part
        for c in range(step // LANES):
            blocks_ref[pl.ds(n // LANES + c, slots, stride=PITCH), :] = total[:, c * LANES : (c + 1) * LANES]
    for s in range(0, slots, 16):
        for r in range(s, s + 16):
            out_ref[r] = blocks_ref[r * PITCH : r * PITCH + chunks, :].astype(BF16)


def expert_answers(arrived, pieces, places):
    slots, chunks, _ = arrived.shape
    width = chunks * LANES
    units = pieces[0].shape[1]
    return pl.pallas_call(
        lambda *refs: expert_kernel(places, *refs),
        out_shape=shape_of(arrived.shape, BF16),
        in_specs=[VMEM] + [ANY] * len(pieces),
        out_specs=VMEM,
        scratch_shapes=[
            pltpu.VMEM((slots * PITCH, LANES), F32),
            pltpu.VMEM((slots, width), BF16),
            pltpu.VMEM((slots, 4 * units), BF16),
            pltpu.VMEM((4, 3 * width, units), BF16),
            pltpu.SemaphoreType.DMA((len(places),)),
        ],
        compiler_params=limit(36),
        name="expert_answers",
    )(held(arrived), *far_off(*pieces))


def enter_kernel(*refs):
    count = (len(refs) - 1) // 2
    sources, tail_ref, targets, sem = refs[:count], refs[count], refs[count + 1 : -1], refs[-1]
    rows = tail_ref.shape[0]
    copies = []
    start = 0
    for n, ref in enumerate((sources[0], sources[1], sources[-1])):
        length, width = ref.shape
        source = ref.at[pl.ds(length - rows, rows)]
        copies.append(pltpu.make_async_copy(source, tail_ref.at[:, pl.ds(start, width)], sem.at[n]))
        start += width
    for n, (source, target) in enumerate(zip(sources[:-1], targets)):
        copies.append(pltpu.make_async_copy(source, target, sem.at[3 + n]))
    for copy in copies:
        copy.start()
    for copy in copies:
        copy.wait()


def entered(rows, values, last):
    width = values[0].shape[1] + values[1].shape[1] + last.shape[1]
    count = len(values)
    return pl.pallas_call(
        enter_kernel,
        out_shape=(near((rows, width), BF16), *(near(value.shape, value.dtype) for value in values)),
        in_specs=[ANY] * (count + 1),
        out_specs=(VMEM,) * (count + 1),
        scratch_shapes=[pltpu.SemaphoreType.DMA((3 + count,))],
        compiler_params=limit(1),
        name="entered",
    )(*far_off(*values, last))


def moved_kernel(moves, *refs):
    count = len(refs) - 5
    sources, targets, stage_ref, into, out = refs[:count], refs[count : count + 2], refs[-3], refs[-2], refs[-1]
    step = stage_ref.shape[1]
    loads, stores = [], []
    for target, parts in zip(targets, moves):
        to = 0
        for which, start, size in parts:
            for at in range(start, start + size, step):
                n = len(loads)
                loads.append(pltpu.make_async_copy(sources[which].at[pl.ds(at, step)], stage_ref.at[n], into.at[n]))
                stores.append(pltpu.make_async_copy(stage_ref.at[n], target.at[pl.ds(to, step)], out.at[n]))
                to += step
    for load in loads:
        load.start()
    for load, store in zip(loads, stores):
        load.wait()
        store.start()
    for store in stores:
        store.wait()


def moved(values, *moves):
    units = values[0].shape[1]
    step = min(size for parts in moves for _, _, size in parts) // 2
    rows = [sum(size for _, _, size in parts) for parts in moves]
    count = sum(rows) // step
    return pl.pallas_call(
        lambda *refs: moved_kernel(moves, *refs),
        out_shape=tuple(pltpu.HBM((size, units), BF16) for size in rows),
        in_specs=[ANY] * len(values),
        out_specs=(ANY,) * len(moves),
        scratch_shapes=[
            pltpu.VMEM((count, step, units), BF16),
            pltpu.SemaphoreType.DMA((count,)),
            pltpu.SemaphoreType.DMA((count,)),
        ],
        compiler_params=limit(12),
        name="moved",
    )(*far_off(*values))


def final_kernel(top_count, returned_ref, middle_ref, slots_ref, weights_ref, gain_ref, bias_ref, out_ref, blocks_ref):
    rows_here, chunks, _ = middle_ref.shape

    def one(r, carry):
        total = returned_ref[slots_ref[0, r]].astype(F32) * weights_ref[0, r]
        for k in range(1, top_count):
            total = total + returned_ref[slots_ref[k, r]].astype(F32) * weights_ref[k, r]
        start = pl.multiple_of(r * chunks, 16)
        blocks_ref[pl.ds(start, chunks), :] = ALPHA * middle_ref[r].astype(F32) + total
        return carry

    lax.fori_loop(0, rows_here, one, 0, unroll=4)
    for r in range(0, rows_here, 16):
        values = jnp.concatenate(
            [blocks_ref[pl.ds(r * chunks + c, 16, stride=chunks), :] for c in range(chunks)], axis=1
        )
        out_ref[r : r + 16, :] = layer_norm(values, gain_ref[...], bias_ref[...]).astype(BF16)


def final_rows(returned, middle, slots, weights, gain, bias, top_count):
    rows_here, chunks, _ = middle.shape
    return pl.pallas_call(
        lambda *refs: final_kernel(top_count, *refs),
        out_shape=shape_of((rows_here, chunks * LANES), BF16),
        in_specs=[VMEM, VMEM, SMEM, SMEM, VMEM, VMEM],
        out_specs=VMEM,
        scratch_shapes=[pltpu.VMEM((rows_here * chunks, LANES), F32)],
        compiler_params=limit(8),
        name="final_rows",
    )(held(returned), middle, slots, weights, gain, bias)


def turned_by(value, distance):
    peers = lax.axis_size("tp")
    return lax.ppermute(value, "tp", [(i, (i + distance) % peers) for i in range(peers)])


def exchanged(value, axis):
    return lax.all_to_all(value, axis, split_axis=0, concat_axis=0, tiled=True)


def shards(
    head_input_values,
    group_input_vectors,
    group_readout_vectors,
    output_gate_values,
    step_size_logits,
    extra_log_decay,
    head_input_filter,
    input_vector_filter,
    readout_vector_filter,
    step_size_bias,
    head_rate_logarithm,
    direct_path_weight,
    group_norm_scale,
    mixer_output_weight,
    residual,
    first_norm_scale,
    first_norm_bias,
    routes,
    routing_weight,
    expert_gate_weight,
    expert_up_weight,
    expert_down_weight,
    final_norm_scale,
    final_norm_bias,
):
    devices = lax.axis_size(SP)
    experts = expert_gate_weight.shape[0] * devices
    rows_here, top_count = routes.shape
    width = residual.shape[1]
    capacity = 5

    own = (expert_gate_weight[0], expert_up_weight[0], expert_down_weight[0])
    ending, *entering = entered(
        8,
        (
            head_input_values,
            group_input_vectors,
            head_input_filter,
            input_vector_filter,
            step_size_logits.T,
            extra_log_decay.T,
            step_size_bias[None],
            head_rate_logarithm[None],
        ),
        group_readout_vectors,
    )
    tail = lax.ppermute(ending, SP, [(i, i + 1) for i in range(devices - 1)])
    gate, up, down = own
    up_behind = turned_by(up, 1)
    up_ahead = turned_by(up, -1)
    gate_behind = turned_by(gate, 1)
    down_ahead = turned_by(down, -1)
    xc, xdt, bc, running, states, message = end_states(tail, *entering)
    met = exchanged(message, SP)
    slots = slot_layout(routes.T, capacity, experts)
    direct = jnp.repeat(direct_path_weight, HEAD_DIM)[None]
    cc, fixed, factor = local_outputs(
        group_readout_vectors,
        tail,
        readout_vector_filter,
        bc,
        xdt,
        xc,
        running,
        states,
        direct,
        output_gate_values,
    )
    incoming = exchanged(chain(met), SP)
    half = width // 2
    low, high = moved((up_behind, up_ahead), ((0, 0, half),), ((1, half, half),))
    up_low = turned_by(low, 1)
    up_high = turned_by(high, -1)
    sums = projected(fixed, factor, cc, incoming, group_norm_scale[None], mixer_output_weight)
    peers = lax.axis_size("tp")
    parts = exchanged(sums.reshape(peers, rows_here, width), "tp")
    onward = moved(
        (gate_behind, down, down_ahead, gate),
        ((0, 0, width), (1, 0, width)),
        ((2, 0, width), (3, 0, width)),
    )
    onward, parts = lax.optimization_barrier((onward, parts))
    last_on = turned_by(onward[0], 1)
    last_back = turned_by(onward[1], -1)
    middle, outgoing = middle_rows(
        parts, residual, first_norm_scale[None], first_norm_bias[None], slots, top_count, experts * capacity
    )
    chunks = width // LANES
    arrived = exchanged(outgoing.reshape(experts, capacity * chunks, LANES), SP)
    answers = expert_answers(
        arrived.reshape(experts * capacity, chunks, LANES),
        (gate, up, down, gate_behind, up_behind, up_ahead, down_ahead, up_low, up_high, last_on, last_back),
        (
            (0, 0, width, 0, 0),
            (1, 0, width, 0, width),
            (2, 0, width, 0, 2 * width),
            (3, 0, width, 1, 0),
            (4, 0, width, 1, width),
            (9, width, width, 1, 2 * width),
            (10, width, width, 2, 0),
            (5, 0, width, 2, width),
            (6, 0, width, 2, 2 * width),
            (9, 0, width, 3, 0),
            (7, 0, half, 3, width),
            (8, 0, half, 3, width + half),
            (10, 0, width, 3, 2 * width),
        ),
    )
    returned = exchanged(answers.reshape(experts, capacity * chunks, LANES), SP)
    return final_rows(
        returned.reshape(experts * capacity, chunks, LANES),
        middle,
        slots,
        routing_weight.T,
        final_norm_scale[None],
        final_norm_bias[None],
        top_count,
    )


def solution(mesh):
    placed = (
        P(SP, "tp"),
        P(SP, "tp"),
        P(SP, "tp"),
        P(SP, "tp"),
        P(SP, "tp"),
        P(SP, "tp"),
        P(None, "tp"),
        P(None, "tp"),
        P(None, "tp"),
        P("tp"),
        P("tp"),
        P("tp"),
        P("tp"),
        P("tp", None),
        P(SP_TP, None),
        P(),
        P(),
        P(SP_TP, None),
        P(SP_TP, None),
        P(SP, None, "tp"),
        P(SP, None, "tp"),
        P(SP, None, "tp"),
        P(),
        P(),
    )
    return jax.shard_map(shards, mesh=mesh, in_specs=placed, out_specs=P(SP_TP, None), check_vma=False)
```

```python
import jax
import jax.numpy as jnp
from jax import lax
from jax.experimental import pallas as pl
from jax.experimental.pallas import tpu as pltpu
from jax.sharding import PartitionSpec as P


HEAD_DIM = 64
STATE_WIDTH = 128
BLOCK = 128
LANES = 128
PITCH = 20
SP = "sp"
SP_TP = ("sp", "tp")
EPS = 1e-05
ALPHA = 8.0**0.25
F32 = jnp.float32
BF16 = jnp.bfloat16

VMEM = pl.BlockSpec(memory_space=pltpu.VMEM)
SMEM = pl.BlockSpec(memory_space=pltpu.SMEM)
ANY = pl.BlockSpec(memory_space=pl.ANY)


def limit(mib):
    return pltpu.CompilerParams(vmem_limit_bytes=mib * 1024 * 1024)


def shape_of(shape, dtype):
    return jax.ShapeDtypeStruct(shape, dtype)


def near(shape, dtype):
    return pltpu.VMEM(shape, dtype)


def held(value):
    return pltpu.with_memory_space_constraint(value, pltpu.VMEM)


def far_off(*values):
    return [pltpu.with_memory_space_constraint(value, pltpu.HBM) for value in values]


def dot(a, b, dims=((1,), (0,))):
    return lax.dot_general(a, b, (dims, ((), ())), preferred_element_type=F32)


def silu(v):
    return 0.5 * v * (1.0 + jnp.tanh(0.5 * v))


def spread_heads(values, group, heads, width):
    total = values.shape[1]
    row = lax.broadcasted_iota(jnp.int32, (total, width), 0)
    col = lax.broadcasted_iota(jnp.int32, (total, width), 1)
    first = group * heads + col // HEAD_DIM
    pick = jnp.where(row == first, 1.0, 0.0).astype(BF16)
    high = values.astype(BF16)
    low = (values - high.astype(F32)).astype(BF16)
    return dot(high, pick) + dot(low, pick)


def fill_rows(rows_ref, tail_ref, raw_ref, cols, offset, length):
    rows_ref[0:8, :] = tail_ref[:, offset + cols.start : offset + cols.stop].astype(F32)
    rows_ref[8 : 8 + length, :] = raw_ref[:, cols].astype(F32)


def conv_cols(rows_ref, taps, length, margin):
    total = taps[0:1, :] * rows_ref[8 - margin : 8 - margin + length, :]
    for k in range(1, margin + 1):
        total = total + taps[k : k + 1, :] * rows_ref[8 - margin + k : 8 - margin + k + length, :]
    return silu(total)


def turned(ref):
    rows, length = ref.shape
    parts = []
    for i in range(0, length, BLOCK):
        tall = jnp.concatenate([ref[:, i : i + BLOCK], jnp.zeros((BLOCK - rows, BLOCK), F32)], axis=0)
        parts.append(tall.T[:, :rows])
    return jnp.concatenate(parts, axis=0)


def log_decays(logits_ref, extra_ref, bias_ref, rate_ref):
    raw = turned(logits_ref) + bias_ref[...]
    step = jnp.maximum(raw, 0.0) + jnp.log1p(jnp.exp(-jnp.abs(raw)))
    return step, -step * jnp.exp(rate_ref[...]) + turned(extra_ref)


def running_sum(block):
    t = lax.broadcasted_iota(jnp.int32, (BLOCK, BLOCK), 0)
    s = lax.broadcasted_iota(jnp.int32, (BLOCK, BLOCK), 1)
    lower = jnp.where(t >= s, 1.0, 0.0)
    return jnp.dot(lower, block, precision=lax.Precision.HIGHEST, preferred_element_type=F32)


def end_state_kernel(
    x_ref,
    b_ref,
    tail_ref,
    xf_ref,
    bf_ref,
    logits_ref,
    extra_ref,
    bias_ref,
    rate_ref,
    xc_ref,
    xdt_ref,
    bc_ref,
    running_ref,
    states_ref,
    message_ref,
    rows_ref,
):
    length, channels = x_ref.shape
    margin = xf_ref.shape[0] - 1
    groups = b_ref.shape[1] // STATE_WIDTH
    width = channels // groups
    heads = width // HEAD_DIM
    blocks = length // BLOCK
    step, decay = log_decays(logits_ref, extra_ref, bias_ref, rate_ref)
    sums = []
    for i in range(blocks):
        part = running_sum(decay[i * BLOCK : (i + 1) * BLOCK])
        running_ref[i * BLOCK : (i + 1) * BLOCK, :] = part
        sums.append(part)
    for c in range(0, groups * STATE_WIDTH, LANES):
        cols = slice(c, c + LANES)
        fill_rows(rows_ref, tail_ref, b_ref, cols, channels, length)
        bc_ref[:, cols] = conv_cols(rows_ref, bf_ref[:, cols].astype(F32), length, margin).astype(BF16)
    for c in range(0, channels, LANES):
        cols = slice(c, c + LANES)
        fill_rows(rows_ref, tail_ref, x_ref, cols, 0, length)
        xc_ref[:, cols] = conv_cols(rows_ref, xf_ref[:, cols].astype(F32), length, margin).astype(BF16)
    total = jnp.zeros((1, decay.shape[1]), F32)
    for i in range(blocks):
        total = total + sums[i][BLOCK - 1 : BLOCK]
    tiles = width // LANES
    for g in range(groups):
        state = None
        for i in range(blocks):
            rows = slice(i * BLOCK, (i + 1) * BLOCK)
            here = slice(g * width, (g + 1) * width)
            ending = sums[i][BLOCK - 1 : BLOCK]
            step_wide = spread_heads(step[rows], g, heads, width)
            left_wide = spread_heads(jnp.exp(ending - sums[i]), g, heads, width)
            scaled = xc_ref[rows, here].astype(F32) * step_wide
            xdt_ref[rows, here] = scaled.astype(BF16)
            keys = bc_ref[rows, g * STATE_WIDTH : (g + 1) * STATE_WIDTH].astype(F32).T.astype(BF16)
            added = dot(keys, (scaled * left_wide).astype(BF16))
            if state is None:
                state = added
            else:
                state = state * spread_heads(jnp.exp(ending), g, heads, width) + added
            if i + 1 < blocks:
                states_ref[i, g] = state
        high = total.astype(BF16)
        rest = total - high.astype(F32)
        low = rest.astype(BF16)
        least = (rest - low.astype(F32)).astype(BF16)
        parts = jnp.concatenate([high, low, least, jnp.zeros((5, total.shape[1]), BF16)], axis=0)
        logs = spread_heads(parts.astype(F32), g, heads, width).astype(BF16)
        for n in range(STATE_WIDTH // 16):
            for p in range(tiles):
                at = (g * (STATE_WIDTH // 16) + n) * tiles + p
                message_ref[at, 0:16, :] = state[n * 16 : (n + 1) * 16, p * LANES : (p + 1) * LANES].astype(BF16)
                message_ref[at, 16:24, :] = logs[:, p * LANES : (p + 1) * LANES]


def end_states(tail, x, b, xf, bf, logits, extra, bias, rate):
    length, channels = x.shape
    groups = b.shape[1] // STATE_WIDTH
    blocks = length // BLOCK
    width = channels // groups
    pieces = groups * STATE_WIDTH * width // (16 * LANES)
    return pl.pallas_call(
        end_state_kernel,
        out_shape=(
            pltpu.HBM((length, channels), BF16),
            pltpu.HBM((length, channels), BF16),
            pltpu.HBM(b.shape, BF16),
            pltpu.HBM((length, logits.shape[0]), F32),
            pltpu.HBM((blocks - 1, groups, STATE_WIDTH, width), F32),
            shape_of((pieces, 24, LANES), BF16),
        ),
        in_specs=[VMEM] * 9,
        out_specs=(VMEM,) * 6,
        scratch_shapes=[pltpu.VMEM((8 + length, LANES), F32)],
        compiler_params=limit(12),
        name="end_states",
    )(*map(held, (x, b, tail, xf, bf, logits, extra, bias, rate)))


def chain_kernel(parts_ref, out_ref):
    peers = parts_ref.shape[0]

    def one(j, state):
        out_ref[j] = state.astype(BF16)
        logs = parts_ref[j, 16:24, :].astype(F32)
        factor = jnp.exp(logs[0:1] + logs[1:2] + logs[2:3])
        return state * factor + parts_ref[j, 0:16, :].astype(F32)

    lax.fori_loop(0, peers, one, jnp.zeros((16, LANES), F32), unroll=8)


def chain(parts):
    return pl.pallas_call(
        chain_kernel,
        out_shape=shape_of((parts.shape[0], 16, LANES), BF16),
        in_specs=[VMEM],
        out_specs=VMEM,
        compiler_params=limit(4),
        name="chain",
    )(held(parts))


def local_kernel(
    c_ref,
    tail_ref,
    cf_ref,
    bc_ref,
    xdt_ref,
    xc_ref,
    running_ref,
    states_ref,
    direct_ref,
    gate_ref,
    cc_ref,
    fixed_ref,
    factor_ref,
    rows_ref,
):
    length, channels = xdt_ref.shape
    margin = cf_ref.shape[0] - 1
    groups = bc_ref.shape[1] // STATE_WIDTH
    width = channels // groups
    heads = width // HEAD_DIM
    offset = channels + groups * STATE_WIDTH
    for c in range(0, groups * STATE_WIDTH, LANES):
        cols = slice(c, c + LANES)
        fill_rows(rows_ref, tail_ref, c_ref, cols, offset, length)
        cc_ref[:, cols] = conv_cols(rows_ref, cf_ref[:, cols].astype(F32), length, margin).astype(BF16)
    t = lax.broadcasted_iota(jnp.int32, (BLOCK, BLOCK), 0)
    s = lax.broadcasted_iota(jnp.int32, (BLOCK, BLOCK), 1)
    causal = t >= s
    first_head = lax.broadcasted_iota(jnp.int32, (BLOCK, LANES), 1) < HEAD_DIM
    started = jnp.zeros((1, running_ref.shape[1]), F32)
    for i in range(length // BLOCK):
        rows = slice(i * BLOCK, (i + 1) * BLOCK)
        running = running_ref[rows, :]
        padded = jnp.concatenate([running, jnp.zeros((BLOCK, BLOCK - running.shape[1]), F32)], axis=1)
        across = padded.T
        since_block = jnp.exp(running)
        since_start = jnp.exp(running + started)
        started = started + running[BLOCK - 1 : BLOCK]
        for g in range(groups):
            here = slice(g * width, (g + 1) * width)
            wide = slice(g * STATE_WIDTH, (g + 1) * STATE_WIDTH)
            products = dot(cc_ref[rows, wide], bc_ref[rows, wide], ((1,), (1,)))
            products = jnp.where(causal, products, 0.0)
            gate = silu(gate_ref[rows, here].astype(F32))
            factor_ref[rows, here] = (spread_heads(since_start, g, heads, width) * gate).astype(BF16)
            carried = None
            if i > 0:
                read = dot(cc_ref[rows, wide], states_ref[i - 1, g].astype(BF16))
                carried = read * spread_heads(since_block, g, heads, width)
            for p in range(width // LANES):
                part = slice(p * LANES, (p + 1) * LANES)
                cols = slice(g * width + p * LANES, g * width + (p + 1) * LANES)
                pair = xdt_ref[rows, cols]
                total = direct_ref[:, cols] * xc_ref[rows, cols].astype(F32)
                if carried is not None:
                    total = total + carried[:, part]
                for q in range(LANES // HEAD_DIM):
                    h = g * heads + p * (LANES // HEAD_DIM) + q
                    spread = running[:, h : h + 1] - across[h : h + 1, :]
                    weights = (products * jnp.exp(jnp.where(causal, spread, 0.0))).astype(BF16)
                    keep = first_head if q == 0 else ~first_head
                    total = total + dot(weights, jnp.where(keep, pair, jnp.zeros_like(pair)))
                fixed_ref[rows, cols] = (total * gate[:, part]).astype(BF16)


def local_outputs(c, tail, cf, bc, xdt, xc, running, states, direct, gate):
    length, channels = xdt.shape
    return pl.pallas_call(
        local_kernel,
        out_shape=(
            near(c.shape, BF16),
            near((length, channels), BF16),
            near((length, channels), BF16),
        ),
        in_specs=[VMEM] * 10,
        out_specs=(VMEM,) * 3,
        scratch_shapes=[pltpu.VMEM((8 + length, LANES), F32)],
        compiler_params=limit(14),
        name="local_outputs",
    )(c, tail, cf, bc, xdt, xc, running, states, direct, gate)


def project_kernel(fixed_ref, factor_ref, cc_ref, incoming_ref, scale_ref, w_hbm, out_ref, w_ref, rows_ref, read_ref, sem):
    copies = [pltpu.make_async_copy(w_hbm.at[:, pl.ds(n * 512, 512)], w_ref.at[n], sem.at[n]) for n in range(4)]
    for copy in copies:
        copy.start()
    length, channels = fixed_ref.shape
    groups = cc_ref.shape[1] // STATE_WIDTH
    width = channels // groups
    tiles = width // LANES
    for g in range(groups):
        here = slice(g * width, (g + 1) * width)
        wide = slice(g * STATE_WIDTH, (g + 1) * STATE_WIDTH)
        lines = []
        for n in range(STATE_WIDTH // 16):
            at = (g * (STATE_WIDTH // 16) + n) * tiles
            lines.append(jnp.concatenate([incoming_ref[at + p] for p in range(tiles)], axis=1))
        incoming = jnp.concatenate(lines, axis=0)
        read_ref[:, here] = dot(cc_ref[:, wide], incoming)
    for g in range(groups):
        here = slice(g * width, (g + 1) * width)
        for i in range(0, length, 16):
            rows = slice(i, i + 16)
            gated = fixed_ref[rows, here].astype(F32) + read_ref[rows, here] * factor_ref[rows, here].astype(F32)
            power = jnp.mean(gated * gated, axis=1, keepdims=True)
            normed = gated * lax.rsqrt(power + EPS) * scale_ref[:, here].astype(F32)
            rows_ref[rows, here] = normed.astype(BF16)
    for n, copy in enumerate(copies):
        copy.wait()
        out_ref[:, n * 512 : (n + 1) * 512] = dot(rows_ref[...], w_ref[n]).astype(BF16)


def projected(fixed, factor, cc, incoming, scale, w):
    length, channels = fixed.shape
    return pl.pallas_call(
        project_kernel,
        out_shape=near((length, w.shape[1]), BF16),
        in_specs=[VMEM] * 5 + [ANY],
        out_specs=VMEM,
        scratch_shapes=[
            pltpu.VMEM((4, w.shape[0], 512), BF16),
            pltpu.VMEM((length, channels), BF16),
            pltpu.VMEM((length, channels), F32),
            pltpu.SemaphoreType.DMA((4,)),
        ],
        compiler_params=limit(20),
        name="projected",
    )(held(fixed), held(factor), held(cc), held(incoming), scale, *far_off(w))


def slots_kernel(capacity, routes_ref, slots_ref, count_ref):
    def clear(e, carry):
        count_ref[e] = 0
        return carry

    lax.fori_loop(0, count_ref.shape[0], clear, 0, unroll=8)

    def one(r, carry):
        for k in range(routes_ref.shape[0]):
            e = routes_ref[k, r]
            used = count_ref[e]
            count_ref[e] = used + 1
            slots_ref[k, r] = e * capacity + used
        return carry

    lax.fori_loop(0, routes_ref.shape[1], one, 0, unroll=4)


def slot_layout(routes, capacity, experts):
    return pl.pallas_call(
        lambda *refs: slots_kernel(capacity, *refs),
        out_shape=shape_of(routes.shape, jnp.int32),
        in_specs=[SMEM],
        out_specs=SMEM,
        scratch_shapes=[pltpu.SMEM((experts,), jnp.int32)],
        compiler_params=limit(1),
        name="slot_layout",
    )(routes)


def layer_norm(values, gain_row, bias_row):
    mean_value = jnp.mean(values, axis=-1, keepdims=True)
    centred = values - mean_value
    spread = jnp.mean(centred * centred, axis=-1, keepdims=True)
    return centred * lax.rsqrt(spread + EPS) * gain_row + bias_row


def middle_kernel(top_count, parts_ref, residual_ref, gain_ref, bias_ref, slots_ref, middle_ref, out_ref, blocks_ref):
    rows_here, width = residual_ref.shape
    chunks = width // LANES
    for r in range(0, rows_here, 16):
        rows = slice(r, r + 16)
        mixed = parts_ref[0, rows, :].astype(F32)
        for k in range(1, parts_ref.shape[0]):
            mixed = mixed + parts_ref[k, rows, :].astype(F32)
        values = layer_norm(ALPHA * residual_ref[rows, :].astype(F32) + mixed, gain_ref[...], bias_ref[...])
        for c in range(chunks):
            blocks_ref[pl.ds(r * PITCH + c, 16, stride=PITCH), :] = values[:, c * LANES : (c + 1) * LANES]

    def one(r, carry):
        at = pl.multiple_of(r * PITCH, 4)
        block = blocks_ref[pl.ds(at, chunks), :].astype(BF16)
        middle_ref[r] = block
        for k in range(top_count):
            out_ref[slots_ref[k, r]] = block
        return carry

    lax.fori_loop(0, rows_here, one, 0, unroll=8)


def middle_rows(parts, residual, gain, bias, slots, top_count, slot_total):
    rows_here, width = residual.shape
    chunks = width // LANES
    return pl.pallas_call(
        lambda *refs: middle_kernel(top_count, *refs),
        out_shape=(
            shape_of((rows_here, chunks, LANES), BF16),
            shape_of((slot_total, chunks, LANES), BF16),
        ),
        in_specs=[VMEM] * 4 + [SMEM],
        out_specs=(VMEM, VMEM),
        scratch_shapes=[pltpu.VMEM((rows_here * PITCH, LANES), F32)],
        compiler_params=limit(8),
        name="middle_rows",
    )(held(parts), residual, gain, bias, slots)


def expert_kernel(places, arrived_ref, *refs):
    pieces = refs[:-6]
    out_ref, blocks_ref, x_ref, hidden_ref, buffer_ref, sem = refs[-6:]
    slots, chunks, _ = arrived_ref.shape
    width = chunks * LANES
    quarters, _, units = buffer_ref.shape
    copies = []
    for n, (which, at, size, quarter, to) in enumerate(places):
        source = pieces[which].at[pl.ds(at, size)]
        copies.append((quarter, pltpu.make_async_copy(source, buffer_ref.at[quarter, pl.ds(to, size)], sem.at[n])))
    for _, copy in copies:
        copy.start()
    for s in range(0, slots, 16):
        for r in range(s, s + 16):
            blocks_ref[r * PITCH : r * PITCH + chunks, :] = arrived_ref[r].astype(F32)
    for c in range(chunks):
        x_ref[:, c * LANES : (c + 1) * LANES] = blocks_ref[pl.ds(c, slots, stride=PITCH), :].astype(BF16)
    for q in range(quarters):
        for quarter, copy in copies:
            if quarter == q:
                copy.wait()
        gate = dot(x_ref[...], buffer_ref[q, :width, :])
        up = dot(x_ref[...], buffer_ref[q, width : 2 * width, :])
        hidden_ref[:, q * units : (q + 1) * units] = (silu(gate) * up).astype(BF16)
    step = 512
    for n in range(0, width, step):
        total = None
        for q in range(quarters):
            down = buffer_ref[q, 2 * width + n : 2 * width + n + step, :]
            part = dot(hidden_ref[:, q * units : (q + 1) * units], down, ((1,), (1,)))
            total = part if total is None else total + part
        for c in range(step // LANES):
            blocks_ref[pl.ds(n // LANES + c, slots, stride=PITCH), :] = total[:, c * LANES : (c + 1) * LANES]
    for s in range(0, slots, 16):
        for r in range(s, s + 16):
            out_ref[r] = blocks_ref[r * PITCH : r * PITCH + chunks, :].astype(BF16)


def expert_answers(arrived, pieces, places):
    slots, chunks, _ = arrived.shape
    width = chunks * LANES
    units = pieces[0].shape[1]
    return pl.pallas_call(
        lambda *refs: expert_kernel(places, *refs),
        out_shape=shape_of(arrived.shape, BF16),
        in_specs=[VMEM] + [ANY] * len(pieces),
        out_specs=VMEM,
        scratch_shapes=[
            pltpu.VMEM((slots * PITCH, LANES), F32),
            pltpu.VMEM((slots, width), BF16),
            pltpu.VMEM((slots, 4 * units), BF16),
            pltpu.VMEM((4, 3 * width, units), BF16),
            pltpu.SemaphoreType.DMA((len(places),)),
        ],
        compiler_params=limit(36),
        name="expert_answers",
    )(held(arrived), *far_off(*pieces))


def enter_kernel(*refs):
    count = (len(refs) - 1) // 2
    sources, tail_ref, targets, sem = refs[:count], refs[count], refs[count + 1 : -1], refs[-1]
    rows = tail_ref.shape[0]
    copies = []
    start = 0
    for n, ref in enumerate((sources[0], sources[1], sources[-1])):
        length, width = ref.shape
        source = ref.at[pl.ds(length - rows, rows)]
        copies.append(pltpu.make_async_copy(source, tail_ref.at[:, pl.ds(start, width)], sem.at[n]))
        start += width
    for n, (source, target) in enumerate(zip(sources[:-1], targets)):
        copies.append(pltpu.make_async_copy(source, target, sem.at[3 + n]))
    for copy in copies:
        copy.start()
    for copy in copies:
        copy.wait()


def entered(rows, values, last):
    width = values[0].shape[1] + values[1].shape[1] + last.shape[1]
    count = len(values)
    return pl.pallas_call(
        enter_kernel,
        out_shape=(near((rows, width), BF16), *(near(value.shape, value.dtype) for value in values)),
        in_specs=[ANY] * (count + 1),
        out_specs=(VMEM,) * (count + 1),
        scratch_shapes=[pltpu.SemaphoreType.DMA((3 + count,))],
        compiler_params=limit(1),
        name="entered",
    )(*far_off(*values, last))


def moved_kernel(moves, *refs):
    count = len(refs) - 5
    sources, targets, stage_ref, into, out = refs[:count], refs[count : count + 2], refs[-3], refs[-2], refs[-1]
    step = stage_ref.shape[1]
    loads, stores = [], []
    for target, parts in zip(targets, moves):
        to = 0
        for which, start, size in parts:
            for at in range(start, start + size, step):
                n = len(loads)
                loads.append(pltpu.make_async_copy(sources[which].at[pl.ds(at, step)], stage_ref.at[n], into.at[n]))
                stores.append(pltpu.make_async_copy(stage_ref.at[n], target.at[pl.ds(to, step)], out.at[n]))
                to += step
    for load in loads:
        load.start()
    for load, store in zip(loads, stores):
        load.wait()
        store.start()
    for store in stores:
        store.wait()


def moved(values, *moves):
    units = values[0].shape[1]
    step = min(size for parts in moves for _, _, size in parts) // 2
    rows = [sum(size for _, _, size in parts) for parts in moves]
    count = sum(rows) // step
    return pl.pallas_call(
        lambda *refs: moved_kernel(moves, *refs),
        out_shape=tuple(pltpu.HBM((size, units), BF16) for size in rows),
        in_specs=[ANY] * len(values),
        out_specs=(ANY,) * len(moves),
        scratch_shapes=[
            pltpu.VMEM((count, step, units), BF16),
            pltpu.SemaphoreType.DMA((count,)),
            pltpu.SemaphoreType.DMA((count,)),
        ],
        compiler_params=limit(12),
        name="moved",
    )(*far_off(*values))


def final_kernel(top_count, returned_ref, middle_ref, slots_ref, weights_ref, gain_ref, bias_ref, out_ref, blocks_ref):
    rows_here, chunks, _ = middle_ref.shape

    def one(r, carry):
        total = returned_ref[slots_ref[0, r]].astype(F32) * weights_ref[0, r]
        for k in range(1, top_count):
            total = total + returned_ref[slots_ref[k, r]].astype(F32) * weights_ref[k, r]
        start = pl.multiple_of(r * PITCH, 4)
        blocks_ref[pl.ds(start, chunks), :] = ALPHA * middle_ref[r].astype(F32) + total
        return carry

    lax.fori_loop(0, rows_here, one, 0, unroll=8)
    for r in range(0, rows_here, 16):
        values = jnp.concatenate(
            [blocks_ref[pl.ds(r * PITCH + c, 16, stride=PITCH), :] for c in range(chunks)], axis=1
        )
        out_ref[r : r + 16, :] = layer_norm(values, gain_ref[...], bias_ref[...]).astype(BF16)


def final_rows(returned, middle, slots, weights, gain, bias, top_count):
    rows_here, chunks, _ = middle.shape
    return pl.pallas_call(
        lambda *refs: final_kernel(top_count, *refs),
        out_shape=shape_of((rows_here, chunks * LANES), BF16),
        in_specs=[VMEM, VMEM, SMEM, SMEM, VMEM, VMEM],
        out_specs=VMEM,
        scratch_shapes=[pltpu.VMEM((rows_here * PITCH, LANES), F32)],
        compiler_params=limit(8),
        name="final_rows",
    )(held(returned), middle, slots, weights, gain, bias)


def turned_by(value, distance):
    peers = lax.axis_size("tp")
    return lax.ppermute(value, "tp", [(i, (i + distance) % peers) for i in range(peers)])


def exchanged(value, axis):
    return lax.all_to_all(value, axis, split_axis=0, concat_axis=0, tiled=True)


def shards(
    head_input_values,
    group_input_vectors,
    group_readout_vectors,
    output_gate_values,
    step_size_logits,
    extra_log_decay,
    head_input_filter,
    input_vector_filter,
    readout_vector_filter,
    step_size_bias,
    head_rate_logarithm,
    direct_path_weight,
    group_norm_scale,
    mixer_output_weight,
    residual,
    first_norm_scale,
    first_norm_bias,
    routes,
    routing_weight,
    expert_gate_weight,
    expert_up_weight,
    expert_down_weight,
    final_norm_scale,
    final_norm_bias,
):
    devices = lax.axis_size(SP)
    experts = expert_gate_weight.shape[0] * devices
    rows_here, top_count = routes.shape
    width = residual.shape[1]
    capacity = 5

    own = (expert_gate_weight[0], expert_up_weight[0], expert_down_weight[0])
    ending, *entering = entered(
        8,
        (
            head_input_values,
            group_input_vectors,
            head_input_filter,
            input_vector_filter,
            step_size_logits.T,
            extra_log_decay.T,
            step_size_bias[None],
            head_rate_logarithm[None],
        ),
        group_readout_vectors,
    )
    tail = lax.ppermute(ending, SP, [(i, i + 1) for i in range(devices - 1)])
    gate, up, down = own
    up_behind = turned_by(up, 1)
    up_ahead = turned_by(up, -1)
    gate_behind = turned_by(gate, 1)
    down_ahead = turned_by(down, -1)
    xc, xdt, bc, running, states, message = end_states(tail, *entering)
    met = exchanged(message, SP)
    slots = slot_layout(routes.T, capacity, experts)
    direct = jnp.repeat(direct_path_weight, HEAD_DIM)[None]
    cc, fixed, factor = local_outputs(
        group_readout_vectors,
        tail,
        readout_vector_filter,
        bc,
        xdt,
        xc,
        running,
        states,
        direct,
        output_gate_values,
    )
    incoming = exchanged(chain(met), SP)
    half = width // 2
    low, high = moved((up_behind, up_ahead), ((0, 0, half),), ((1, half, half),))
    up_low = turned_by(low, 1)
    up_high = turned_by(high, -1)
    sums = projected(fixed, factor, cc, incoming, group_norm_scale[None], mixer_output_weight)
    peers = lax.axis_size("tp")
    parts = exchanged(sums.reshape(peers, rows_here, width), "tp")
    onward = moved(
        (gate_behind, down, down_ahead, gate),
        ((0, 0, width), (1, 0, width)),
        ((2, 0, width), (3, 0, width)),
    )
    onward, parts = lax.optimization_barrier((onward, parts))
    last_on = turned_by(onward[0], 1)
    last_back = turned_by(onward[1], -1)
    middle, outgoing = middle_rows(
        parts, residual, first_norm_scale[None], first_norm_bias[None], slots, top_count, experts * capacity
    )
    chunks = width // LANES
    arrived = exchanged(outgoing.reshape(experts, capacity * chunks, LANES), SP)
    answers = expert_answers(
        arrived.reshape(experts * capacity, chunks, LANES),
        (gate, up, down, gate_behind, up_behind, up_ahead, down_ahead, up_low, up_high, last_on, last_back),
        (
            (0, 0, width, 0, 0),
            (1, 0, width, 0, width),
            (2, 0, width, 0, 2 * width),
            (3, 0, width, 1, 0),
            (4, 0, width, 1, width),
            (9, width, width, 1, 2 * width),
            (10, width, width, 2, 0),
            (5, 0, width, 2, width),
            (6, 0, width, 2, 2 * width),
            (9, 0, width, 3, 0),
            (7, 0, half, 3, width),
            (8, 0, half, 3, width + half),
            (10, 0, width, 3, 2 * width),
        ),
    )
    returned = exchanged(answers.reshape(experts, capacity * chunks, LANES), SP)
    return final_rows(
        returned.reshape(experts * capacity, chunks, LANES),
        middle,
        slots,
        routing_weight.T,
        final_norm_scale[None],
        final_norm_bias[None],
        top_count,
    )


def solution(mesh):
    placed = (
        P(SP, "tp"),
        P(SP, "tp"),
        P(SP, "tp"),
        P(SP, "tp"),
        P(SP, "tp"),
        P(SP, "tp"),
        P(None, "tp"),
        P(None, "tp"),
        P(None, "tp"),
        P("tp"),
        P("tp"),
        P("tp"),
        P("tp"),
        P("tp", None),
        P(SP_TP, None),
        P(),
        P(),
        P(SP_TP, None),
        P(SP_TP, None),
        P(SP, None, "tp"),
        P(SP, None, "tp"),
        P(SP, None, "tp"),
        P(),
        P(),
    )
    return jax.shard_map(shards, mesh=mesh, in_specs=placed, out_specs=P(SP_TP, None), check_vma=False)
```

```python
import math

import jax
import jax.numpy as jnp
from jax import lax
from jax.experimental import pallas as pl
from jax.experimental.pallas import tpu as pltpu
from jax.sharding import PartitionSpec as P


HEAD_DIM = 64
STATE_WIDTH = 128
BLOCK = 128
LANES = 128
PITCH = 20
SP = "sp"
SP_TP = ("sp", "tp")
EPS = 1e-05
ALPHA = 8.0**0.25
F32 = jnp.float32
BF16 = jnp.bfloat16

VMEM = pl.BlockSpec(memory_space=pltpu.VMEM)
SMEM = pl.BlockSpec(memory_space=pltpu.SMEM)
ANY = pl.BlockSpec(memory_space=pl.ANY)


def limit(mib):
    return pltpu.CompilerParams(vmem_limit_bytes=mib * 1024 * 1024)


def shape_of(shape, dtype):
    return jax.ShapeDtypeStruct(shape, dtype)


def near(shape, dtype):
    return pltpu.VMEM(shape, dtype)


def held(value):
    return pltpu.with_memory_space_constraint(value, pltpu.VMEM)


def far_off(*values):
    return [pltpu.with_memory_space_constraint(value, pltpu.HBM) for value in values]


def dot(a, b, dims=((1,), (0,))):
    return lax.dot_general(a, b, (dims, ((), ())), preferred_element_type=F32)


def silu(v):
    return 0.5 * v * (1.0 + jnp.tanh(0.5 * v))


def spread_heads(values, group, heads, width):
    total = values.shape[1]
    row = lax.broadcasted_iota(jnp.int32, (total, width), 0)
    col = lax.broadcasted_iota(jnp.int32, (total, width), 1)
    first = group * heads + col // HEAD_DIM
    pick = jnp.where(row == first, 1.0, 0.0).astype(BF16)
    high = values.astype(BF16)
    low = (values - high.astype(F32)).astype(BF16)
    return dot(high, pick) + dot(low, pick)


def fill_rows(rows_ref, tail_ref, raw_ref, cols, offset, length):
    rows_ref[0:8, :] = tail_ref[:, offset + cols.start : offset + cols.stop].astype(F32)
    rows_ref[8 : 8 + length, :] = raw_ref[:, cols].astype(F32)


def conv_cols(rows_ref, taps, length, margin):
    total = taps[0:1, :] * rows_ref[8 - margin : 8 - margin + length, :]
    for k in range(1, margin + 1):
        total = total + taps[k : k + 1, :] * rows_ref[8 - margin + k : 8 - margin + k + length, :]
    return silu(total)


def turned(ref):
    rows, length = ref.shape
    parts = []
    for i in range(0, length, BLOCK):
        tall = jnp.concatenate([ref[:, i : i + BLOCK], jnp.zeros((BLOCK - rows, BLOCK), F32)], axis=0)
        parts.append(tall.T[:, :rows])
    return jnp.concatenate(parts, axis=0)


def log_decays(logits_ref, extra_ref, bias_ref, rate_ref):
    raw = turned(logits_ref) + bias_ref[...]
    step = jnp.maximum(raw, 0.0) + jnp.log1p(jnp.exp(-jnp.abs(raw)))
    return step, -step * jnp.exp(rate_ref[...]) + turned(extra_ref)


def running_sum(block):
    t = lax.broadcasted_iota(jnp.int32, (BLOCK, BLOCK), 0)
    s = lax.broadcasted_iota(jnp.int32, (BLOCK, BLOCK), 1)
    lower = jnp.where(t >= s, 1.0, 0.0)
    return jnp.dot(lower, block, precision=lax.Precision.HIGHEST, preferred_element_type=F32)


def end_state_kernel(
    x_ref,
    b_ref,
    tail_ref,
    xf_ref,
    bf_ref,
    logits_ref,
    extra_ref,
    bias_ref,
    rate_ref,
    bc_ref,
    running_ref,
    states_ref,
    message_ref,
    xc_ref,
    rows_ref,
):
    length, channels = x_ref.shape
    margin = xf_ref.shape[0] - 1
    groups = b_ref.shape[1] // STATE_WIDTH
    width = channels // groups
    heads = width // HEAD_DIM
    blocks = length // BLOCK
    step, decay = log_decays(logits_ref, extra_ref, bias_ref, rate_ref)
    sums = []
    for i in range(blocks):
        rows = slice(i * BLOCK, (i + 1) * BLOCK)
        part = running_sum(decay[rows])
        running_ref[0, rows, :] = part
        running_ref[1, rows, :] = step[rows]
        sums.append(part)
    for c in range(0, groups * STATE_WIDTH, LANES):
        cols = slice(c, c + LANES)
        fill_rows(rows_ref, tail_ref, b_ref, cols, channels, length)
        bc_ref[:, cols] = conv_cols(rows_ref, bf_ref[:, cols].astype(F32), length, margin).astype(BF16)
    for c in range(0, channels, LANES):
        cols = slice(c, c + LANES)
        fill_rows(rows_ref, tail_ref, x_ref, cols, 0, length)
        xc_ref[:, cols] = conv_cols(rows_ref, xf_ref[:, cols].astype(F32), length, margin).astype(BF16)
    total = jnp.zeros((1, decay.shape[1]), F32)
    for i in range(blocks):
        total = total + sums[i][BLOCK - 1 : BLOCK]
    tiles = width // LANES
    for g in range(groups):
        state = None
        for i in range(blocks):
            rows = slice(i * BLOCK, (i + 1) * BLOCK)
            here = slice(g * width, (g + 1) * width)
            ending = sums[i][BLOCK - 1 : BLOCK]
            step_wide = spread_heads(step[rows], g, heads, width)
            left_wide = spread_heads(jnp.exp(ending - sums[i]), g, heads, width)
            scaled = xc_ref[rows, here].astype(F32) * step_wide
            keys = bc_ref[rows, g * STATE_WIDTH : (g + 1) * STATE_WIDTH].astype(F32).T.astype(BF16)
            added = dot(keys, (scaled * left_wide).astype(BF16))
            if state is None:
                state = added
            else:
                state = state * spread_heads(jnp.exp(ending), g, heads, width) + added
            if i + 1 < blocks:
                states_ref[i, g] = state.astype(BF16)
        high = total.astype(BF16)
        rest = total - high.astype(F32)
        low = rest.astype(BF16)
        least = (rest - low.astype(F32)).astype(BF16)
        parts = jnp.concatenate([high, low, least, jnp.zeros((5, total.shape[1]), BF16)], axis=0)
        logs = spread_heads(parts.astype(F32), g, heads, width).astype(BF16)
        for n in range(STATE_WIDTH // 16):
            for p in range(tiles):
                at = (g * (STATE_WIDTH // 16) + n) * tiles + p
                message_ref[at, 0:16, :] = state[n * 16 : (n + 1) * 16, p * LANES : (p + 1) * LANES].astype(BF16)
                message_ref[at, 16:24, :] = logs[:, p * LANES : (p + 1) * LANES]


def end_states(tail, x, b, xf, bf, logits, extra, bias, rate):
    length, channels = x.shape
    groups = b.shape[1] // STATE_WIDTH
    blocks = length // BLOCK
    width = channels // groups
    pieces = groups * STATE_WIDTH * width // (16 * LANES)
    return pl.pallas_call(
        end_state_kernel,
        out_shape=(
            pltpu.HBM(b.shape, BF16),
            pltpu.HBM((2, length, logits.shape[0]), F32),
            pltpu.HBM((blocks - 1, groups, STATE_WIDTH, width), BF16),
            near((pieces, 24, LANES), BF16),
        ),
        in_specs=[VMEM] * 9,
        out_specs=(VMEM,) * 4,
        scratch_shapes=[pltpu.VMEM((length, channels), BF16), pltpu.VMEM((8 + length, LANES), F32)],
        compiler_params=limit(12),
        name="end_states",
    )(*map(held, (x, b, tail, xf, bf, logits, extra, bias, rate)))


def chain_kernel(parts_ref, out_ref):
    peers = parts_ref.shape[0]

    def one(j, state):
        out_ref[j] = state.astype(BF16)
        logs = parts_ref[j, 16:24, :].astype(F32)
        factor = jnp.exp(logs[0:1] + logs[1:2] + logs[2:3])
        return state * factor + parts_ref[j, 0:16, :].astype(F32)

    lax.fori_loop(0, peers, one, jnp.zeros((16, LANES), F32), unroll=8)


def chain(parts):
    return pl.pallas_call(
        chain_kernel,
        out_shape=shape_of((parts.shape[0], 16, LANES), BF16),
        in_specs=[VMEM],
        out_specs=VMEM,
        compiler_params=limit(4),
        name="chain",
    )(held(parts))


def local_kernel(
    c_ref,
    tail_ref,
    cf_ref,
    bc_ref,
    x_ref,
    xf_ref,
    running_ref,
    states_ref,
    direct_ref,
    gate_ref,
    cc_ref,
    fixed_ref,
    factor_ref,
    xc_ref,
    rows_ref,
):
    length, channels = x_ref.shape
    margin = cf_ref.shape[0] - 1
    groups = bc_ref.shape[1] // STATE_WIDTH
    width = channels // groups
    heads = width // HEAD_DIM
    offset = channels + groups * STATE_WIDTH
    for c in range(0, groups * STATE_WIDTH, LANES):
        cols = slice(c, c + LANES)
        fill_rows(rows_ref, tail_ref, c_ref, cols, offset, length)
        cc_ref[:, cols] = conv_cols(rows_ref, cf_ref[:, cols].astype(F32), length, margin).astype(BF16)
    for c in range(0, channels, LANES):
        cols = slice(c, c + LANES)
        fill_rows(rows_ref, tail_ref, x_ref, cols, 0, length)
        xc_ref[:, cols] = conv_cols(rows_ref, xf_ref[:, cols].astype(F32), length, margin).astype(BF16)
    t = lax.broadcasted_iota(jnp.int32, (BLOCK, BLOCK), 0)
    s = lax.broadcasted_iota(jnp.int32, (BLOCK, BLOCK), 1)
    causal = t >= s
    first_head = lax.broadcasted_iota(jnp.int32, (BLOCK, LANES), 1) < HEAD_DIM
    started = jnp.zeros((1, running_ref.shape[2]), F32)
    for i in range(length // BLOCK):
        rows = slice(i * BLOCK, (i + 1) * BLOCK)
        running, step = running_ref[0, rows, :], running_ref[1, rows, :]
        padded = jnp.concatenate([running, jnp.zeros((BLOCK, BLOCK - running.shape[1]), F32)], axis=1)
        across = padded.T
        since_block = jnp.exp(running)
        since_start = jnp.exp(running + started)
        started = started + running[BLOCK - 1 : BLOCK]
        for g in range(groups):
            here = slice(g * width, (g + 1) * width)
            wide = slice(g * STATE_WIDTH, (g + 1) * STATE_WIDTH)
            products = dot(cc_ref[rows, wide], bc_ref[rows, wide], ((1,), (1,)))
            products = jnp.where(causal, products, 0.0)
            gate = silu(gate_ref[rows, here].astype(F32))
            factor_ref[rows, here] = (spread_heads(since_start, g, heads, width) * gate).astype(BF16)
            inputs = xc_ref[rows, here].astype(F32)
            scaled = (inputs * spread_heads(step, g, heads, width)).astype(BF16)
            carried = None
            if i > 0:
                read = dot(cc_ref[rows, wide], states_ref[i - 1, g])
                carried = read * spread_heads(since_block, g, heads, width)
            for p in range(width // LANES):
                part = slice(p * LANES, (p + 1) * LANES)
                cols = slice(g * width + p * LANES, g * width + (p + 1) * LANES)
                pair = scaled[:, part]
                total = direct_ref[:, cols] * inputs[:, part]
                if carried is not None:
                    total = total + carried[:, part]
                for q in range(LANES // HEAD_DIM):
                    h = g * heads + p * (LANES // HEAD_DIM) + q
                    spread = running[:, h : h + 1] - across[h : h + 1, :]
                    weights = (products * jnp.exp(jnp.where(causal, spread, 0.0))).astype(BF16)
                    keep = first_head if q == 0 else ~first_head
                    total = total + dot(weights, jnp.where(keep, pair, jnp.zeros_like(pair)))
                fixed_ref[rows, cols] = (total * gate[:, part]).astype(BF16)


def local_outputs(c, tail, cf, bc, x, xf, running, states, direct, gate):
    length, channels = x.shape
    return pl.pallas_call(
        local_kernel,
        out_shape=(
            near(c.shape, BF16),
            near((length, channels), BF16),
            near((length, channels), BF16),
        ),
        in_specs=[VMEM] * 10,
        out_specs=(VMEM,) * 3,
        scratch_shapes=[pltpu.VMEM((length, channels), BF16), pltpu.VMEM((8 + length, LANES), F32)],
        compiler_params=limit(14),
        name="local_outputs",
    )(c, tail, cf, bc, x, xf, running, states, direct, gate)


def project_kernel(fixed_ref, factor_ref, cc_ref, incoming_ref, scale_ref, w_hbm, out_ref, w_ref, rows_ref, read_ref, sem):
    copies = [pltpu.make_async_copy(w_hbm.at[:, pl.ds(n * 512, 512)], w_ref.at[n], sem.at[n]) for n in range(4)]
    for copy in copies:
        copy.start()
    length, channels = fixed_ref.shape
    groups = cc_ref.shape[1] // STATE_WIDTH
    width = channels // groups
    tiles = width // LANES
    for g in range(groups):
        here = slice(g * width, (g + 1) * width)
        wide = slice(g * STATE_WIDTH, (g + 1) * STATE_WIDTH)
        lines = []
        for n in range(STATE_WIDTH // 16):
            at = (g * (STATE_WIDTH // 16) + n) * tiles
            lines.append(jnp.concatenate([incoming_ref[at + p] for p in range(tiles)], axis=1))
        incoming = jnp.concatenate(lines, axis=0)
        read_ref[:, here] = dot(cc_ref[:, wide], incoming)
    for g in range(groups):
        here = slice(g * width, (g + 1) * width)
        for i in range(0, length, 16):
            rows = slice(i, i + 16)
            gated = fixed_ref[rows, here].astype(F32) + read_ref[rows, here] * factor_ref[rows, here].astype(F32)
            power = jnp.mean(gated * gated, axis=1, keepdims=True)
            normed = gated * lax.rsqrt(power + EPS) * scale_ref[:, here].astype(F32)
            rows_ref[rows, here] = normed.astype(BF16)
    for n, copy in enumerate(copies):
        copy.wait()
        out_ref[:, n * 512 : (n + 1) * 512] = dot(rows_ref[...], w_ref[n]).astype(BF16)


def projected(fixed, factor, cc, incoming, scale, w):
    length, channels = fixed.shape
    return pl.pallas_call(
        project_kernel,
        out_shape=near((length, w.shape[1]), BF16),
        in_specs=[VMEM] * 5 + [ANY],
        out_specs=VMEM,
        scratch_shapes=[
            pltpu.VMEM((4, w.shape[0], 512), BF16),
            pltpu.VMEM((length, channels), BF16),
            pltpu.VMEM((length, channels), F32),
            pltpu.SemaphoreType.DMA((4,)),
        ],
        compiler_params=limit(20),
        name="projected",
    )(held(fixed), held(factor), held(cc), held(incoming), scale, *far_off(w))


def slots_kernel(capacity, routes_ref, slots_ref, count_ref):
    def clear(e, carry):
        count_ref[e] = 0
        return carry

    lax.fori_loop(0, count_ref.shape[0], clear, 0, unroll=8)

    def one(r, carry):
        for k in range(routes_ref.shape[0]):
            e = routes_ref[k, r]
            used = count_ref[e]
            count_ref[e] = used + 1
            slots_ref[k, r] = e * capacity + used
        return carry

    lax.fori_loop(0, routes_ref.shape[1], one, 0, unroll=4)


def slot_layout(routes, capacity, experts):
    return pl.pallas_call(
        lambda *refs: slots_kernel(capacity, *refs),
        out_shape=shape_of(routes.shape, jnp.int32),
        in_specs=[SMEM],
        out_specs=SMEM,
        scratch_shapes=[pltpu.SMEM((experts,), jnp.int32)],
        compiler_params=limit(1),
        name="slot_layout",
    )(routes)


def layer_norm(values, gain_row, bias_row):
    mean_value = jnp.mean(values, axis=-1, keepdims=True)
    centred = values - mean_value
    spread = jnp.mean(centred * centred, axis=-1, keepdims=True)
    return centred * lax.rsqrt(spread + EPS) * gain_row + bias_row


def middle_kernel(top_count, parts_ref, residual_ref, gain_ref, bias_ref, slots_ref, middle_ref, out_ref, blocks_ref):
    rows_here, width = residual_ref.shape
    chunks = width // LANES
    for r in range(0, rows_here, 16):
        rows = slice(r, r + 16)
        mixed = parts_ref[0, rows, :].astype(F32)
        for k in range(1, parts_ref.shape[0]):
            mixed = mixed + parts_ref[k, rows, :].astype(F32)
        values = layer_norm(ALPHA * residual_ref[rows, :].astype(F32) + mixed, gain_ref[...], bias_ref[...])
        for c in range(chunks):
            blocks_ref[pl.ds(r * PITCH + c, 16, stride=PITCH), :] = values[:, c * LANES : (c + 1) * LANES]

    def one(r, carry):
        at = pl.multiple_of(r * PITCH, 4)
        block = blocks_ref[pl.ds(at, chunks), :].astype(BF16)
        middle_ref[r] = block
        for k in range(top_count):
            out_ref[slots_ref[k, r]] = block
        return carry

    lax.fori_loop(0, rows_here, one, 0, unroll=8)


def middle_rows(parts, residual, gain, bias, slots, top_count, slot_total):
    rows_here, width = residual.shape
    chunks = width // LANES
    return pl.pallas_call(
        lambda *refs: middle_kernel(top_count, *refs),
        out_shape=(
            shape_of((rows_here, chunks, LANES), BF16),
            shape_of((slot_total, chunks, LANES), BF16),
        ),
        in_specs=[VMEM] * 4 + [SMEM],
        out_specs=(VMEM, VMEM),
        scratch_shapes=[pltpu.VMEM((rows_here * PITCH, LANES), F32)],
        compiler_params=limit(8),
        name="middle_rows",
    )(held(parts), residual, gain, bias, slots)


def expert_kernel(places, arrived_ref, *refs):
    pieces = refs[:-6]
    out_ref, blocks_ref, x_ref, hidden_ref, buffer_ref, sem = refs[-6:]
    slots, chunks, _ = arrived_ref.shape
    width = chunks * LANES
    quarters, _, units = buffer_ref.shape
    copies = []
    ordered = sorted(places, key=lambda place: place[4] >= 2 * width)
    for n, (which, at, size, quarter, to) in enumerate(ordered):
        source = pieces[which].at[pl.ds(at, size)]
        copy = pltpu.make_async_copy(source, buffer_ref.at[quarter, pl.ds(to, size)], sem.at[n])
        copies.append((quarter if to < 2 * width else quarters, copy))
    for _, copy in copies:
        copy.start()
    for s in range(0, slots, 16):
        for r in range(s, s + 16):
            blocks_ref[r * PITCH : r * PITCH + chunks, :] = arrived_ref[r].astype(F32)
    for c in range(chunks):
        x_ref[:, c * LANES : (c + 1) * LANES] = blocks_ref[pl.ds(c, slots, stride=PITCH), :].astype(BF16)
    for q in range(quarters):
        for quarter, copy in copies:
            if quarter == q:
                copy.wait()
        gate = dot(x_ref[...], buffer_ref[q, :width, :])
        up = dot(x_ref[...], buffer_ref[q, width : 2 * width, :])
        hidden_ref[:, q * units : (q + 1) * units] = (silu(gate) * up).astype(BF16)
    for quarter, copy in copies:
        if quarter == quarters:
            copy.wait()
    step = 512
    for n in range(0, width, step):
        total = None
        for q in range(quarters):
            down = buffer_ref[q, 2 * width + n : 2 * width + n + step, :]
            part = dot(hidden_ref[:, q * units : (q + 1) * units], down, ((1,), (1,)))
            total = part if total is None else total + part
        for c in range(step // LANES):
            blocks_ref[pl.ds(n // LANES + c, slots, stride=PITCH), :] = total[:, c * LANES : (c + 1) * LANES]
    for s in range(0, slots, 16):
        for r in range(s, s + 16):
            out_ref[r] = blocks_ref[r * PITCH : r * PITCH + chunks, :].astype(BF16)


def expert_answers(arrived, pieces, places):
    slots, chunks, _ = arrived.shape
    width = chunks * LANES
    units = pieces[0].shape[1]
    return pl.pallas_call(
        lambda *refs: expert_kernel(places, *refs),
        out_shape=shape_of(arrived.shape, BF16),
        in_specs=[VMEM] + [ANY] * len(pieces),
        out_specs=VMEM,
        scratch_shapes=[
            pltpu.VMEM((slots * PITCH, LANES), F32),
            pltpu.VMEM((slots, width), BF16),
            pltpu.VMEM((slots, 4 * units), BF16),
            pltpu.VMEM((4, 3 * width, units), BF16),
            pltpu.SemaphoreType.DMA((len(places),)),
        ],
        compiler_params=limit(36),
        name="expert_answers",
    )(held(arrived), *far_off(*pieces))


def enter_kernel(*refs):
    count = (len(refs) - 1) // 2
    sources, tail_ref, targets, sem = refs[:count], refs[count], refs[count + 1 : -1], refs[-1]
    rows = tail_ref.shape[0]
    copies = []
    start = 0
    for n, ref in enumerate((sources[0], sources[1], sources[-1])):
        length, width = ref.shape
        source = ref.at[pl.ds(length - rows, rows)]
        copies.append(pltpu.make_async_copy(source, tail_ref.at[:, pl.ds(start, width)], sem.at[n]))
        start += width
    for n, (source, target) in enumerate(zip(sources[:-1], targets)):
        copies.append(pltpu.make_async_copy(source, target, sem.at[3 + n]))
    for copy in copies:
        copy.start()
    for copy in copies:
        copy.wait()


def entered(rows, values, last):
    width = values[0].shape[1] + values[1].shape[1] + last.shape[1]
    count = len(values)
    return pl.pallas_call(
        enter_kernel,
        out_shape=(near((rows, width), BF16), *(near(value.shape, value.dtype) for value in values)),
        in_specs=[ANY] * (count + 1),
        out_specs=(VMEM,) * (count + 1),
        scratch_shapes=[pltpu.SemaphoreType.DMA((3 + count,))],
        compiler_params=limit(1),
        name="entered",
    )(*far_off(*values, last))


def moved_kernel(moves, *refs):
    count = len(refs) - 5
    sources, targets, stage_ref, into, out = refs[:count], refs[count : count + 2], refs[-3], refs[-2], refs[-1]
    step = stage_ref.shape[1]
    loads, stores = [], []
    for target, parts in zip(targets, moves):
        to = 0
        for which, start, size in parts:
            for at in range(start, start + size, step):
                n = len(loads)
                loads.append(pltpu.make_async_copy(sources[which].at[pl.ds(at, step)], stage_ref.at[n], into.at[n]))
                stores.append(pltpu.make_async_copy(stage_ref.at[n], target.at[pl.ds(to, step)], out.at[n]))
                to += step
    for load in loads:
        load.start()
    for load, store in zip(loads, stores):
        load.wait()
        store.start()
    for store in stores:
        store.wait()


def moved(values, *moves):
    units = values[0].shape[1]
    step = math.gcd(*(size for parts in moves for _, _, size in parts))
    rows = [sum(size for _, _, size in parts) for parts in moves]
    count = sum(rows) // step
    return pl.pallas_call(
        lambda *refs: moved_kernel(moves, *refs),
        out_shape=tuple(pltpu.HBM((size, units), BF16) for size in rows),
        in_specs=[ANY] * len(values),
        out_specs=(ANY,) * len(moves),
        scratch_shapes=[
            pltpu.VMEM((count, step, units), BF16),
            pltpu.SemaphoreType.DMA((count,)),
            pltpu.SemaphoreType.DMA((count,)),
        ],
        compiler_params=limit(12),
        name="moved",
    )(*far_off(*values))


def final_kernel(top_count, returned_ref, middle_ref, slots_ref, weights_ref, gain_ref, bias_ref, out_ref, blocks_ref):
    rows_here, chunks, _ = middle_ref.shape

    def one(r, carry):
        total = returned_ref[slots_ref[0, r]].astype(F32) * weights_ref[0, r]
        for k in range(1, top_count):
            total = total + returned_ref[slots_ref[k, r]].astype(F32) * weights_ref[k, r]
        start = pl.multiple_of(r * PITCH, 4)
        blocks_ref[pl.ds(start, chunks), :] = ALPHA * middle_ref[r].astype(F32) + total
        return carry

    lax.fori_loop(0, rows_here, one, 0, unroll=8)
    for r in range(0, rows_here, 16):
        values = jnp.concatenate(
            [blocks_ref[pl.ds(r * PITCH + c, 16, stride=PITCH), :] for c in range(chunks)], axis=1
        )
        out_ref[r : r + 16, :] = layer_norm(values, gain_ref[...], bias_ref[...]).astype(BF16)


def final_rows(returned, middle, slots, weights, gain, bias, top_count):
    rows_here, chunks, _ = middle.shape
    return pl.pallas_call(
        lambda *refs: final_kernel(top_count, *refs),
        out_shape=shape_of((rows_here, chunks * LANES), BF16),
        in_specs=[VMEM, VMEM, SMEM, SMEM, VMEM, VMEM],
        out_specs=VMEM,
        scratch_shapes=[pltpu.VMEM((rows_here * PITCH, LANES), F32)],
        compiler_params=limit(8),
        name="final_rows",
    )(held(returned), middle, slots, weights, gain, bias)


def turned_by(value, distance):
    peers = lax.axis_size("tp")
    return lax.ppermute(value, "tp", [(i, (i + distance) % peers) for i in range(peers)])


def exchanged(value, axis):
    return lax.all_to_all(value, axis, split_axis=0, concat_axis=0, tiled=True)


def shards(
    head_input_values,
    group_input_vectors,
    group_readout_vectors,
    output_gate_values,
    step_size_logits,
    extra_log_decay,
    head_input_filter,
    input_vector_filter,
    readout_vector_filter,
    step_size_bias,
    head_rate_logarithm,
    direct_path_weight,
    group_norm_scale,
    mixer_output_weight,
    residual,
    first_norm_scale,
    first_norm_bias,
    routes,
    routing_weight,
    expert_gate_weight,
    expert_up_weight,
    expert_down_weight,
    final_norm_scale,
    final_norm_bias,
):
    devices = lax.axis_size(SP)
    experts = expert_gate_weight.shape[0] * devices
    rows_here, top_count = routes.shape
    width = residual.shape[1]
    capacity = 5

    own = (expert_gate_weight[0], expert_up_weight[0], expert_down_weight[0])
    ending, *entering = entered(
        8,
        (
            head_input_values,
            group_input_vectors,
            head_input_filter,
            input_vector_filter,
            step_size_logits.T,
            extra_log_decay.T,
            step_size_bias[None],
            head_rate_logarithm[None],
        ),
        group_readout_vectors,
    )
    tail = lax.ppermute(ending, SP, [(i, i + 1) for i in range(devices - 1)])
    gate, up, down = own
    up_behind = turned_by(up, 1)
    up_ahead = turned_by(up, -1)
    gate_behind = turned_by(gate, 1)
    down_ahead = turned_by(down, -1)
    bc, running, states, message = end_states(tail, *entering)
    met = exchanged(message, SP)
    slots = slot_layout(routes.T, capacity, experts)
    direct = jnp.repeat(direct_path_weight, HEAD_DIM)[None]
    cc, fixed, factor = local_outputs(
        group_readout_vectors,
        tail,
        readout_vector_filter,
        bc,
        head_input_values,
        head_input_filter,
        running,
        states,
        direct,
        output_gate_values,
    )
    incoming = exchanged(chain(met), SP)
    half = width // 2
    extra = width // 8
    low, high = moved(
        (up_behind, down, up_ahead, gate),
        ((0, 0, half), (1, 0, extra)),
        ((2, half, half), (3, 0, extra)),
    )
    up_low = turned_by(low, 1)
    up_high = turned_by(high, -1)
    sums = projected(fixed, factor, cc, incoming, group_norm_scale[None], mixer_output_weight)
    peers = lax.axis_size("tp")
    parts = exchanged(sums.reshape(peers, rows_here, width), "tp")
    onward = moved(
        (gate_behind, down, down_ahead, gate),
        ((0, 0, width), (1, extra, width - extra)),
        ((2, 0, width), (3, extra, width - extra)),
    )
    onward, parts = lax.optimization_barrier((onward, parts))
    last_on = turned_by(onward[0], 1)
    last_back = turned_by(onward[1], -1)
    middle, outgoing = middle_rows(
        parts, residual, first_norm_scale[None], first_norm_bias[None], slots, top_count, experts * capacity
    )
    chunks = width // LANES
    arrived = exchanged(outgoing.reshape(experts, capacity * chunks, LANES), SP)
    answers = expert_answers(
        arrived.reshape(experts * capacity, chunks, LANES),
        (gate, up, down, gate_behind, up_behind, up_ahead, down_ahead, up_low, up_high, last_on, last_back),
        (
            (0, 0, width, 0, 0),
            (1, 0, width, 0, width),
            (2, 0, width, 0, 2 * width),
            (3, 0, width, 1, 0),
            (4, 0, width, 1, width),
            (7, half, extra, 1, 2 * width),
            (9, width, width - extra, 1, 2 * width + extra),
            (8, half, extra, 2, 0),
            (10, width, width - extra, 2, extra),
            (5, 0, width, 2, width),
            (6, 0, width, 2, 2 * width),
            (9, 0, width, 3, 0),
            (7, 0, half, 3, width),
            (8, 0, half, 3, width + half),
            (10, 0, width, 3, 2 * width),
        ),
    )
    returned = exchanged(answers.reshape(experts, capacity * chunks, LANES), SP)
    return final_rows(
        returned.reshape(experts * capacity, chunks, LANES),
        middle,
        slots,
        routing_weight.T,
        final_norm_scale[None],
        final_norm_bias[None],
        top_count,
    )


def solution(mesh):
    placed = (
        P(SP, "tp"),
        P(SP, "tp"),
        P(SP, "tp"),
        P(SP, "tp"),
        P(SP, "tp"),
        P(SP, "tp"),
        P(None, "tp"),
        P(None, "tp"),
        P(None, "tp"),
        P("tp"),
        P("tp"),
        P("tp"),
        P("tp"),
        P("tp", None),
        P(SP_TP, None),
        P(),
        P(),
        P(SP_TP, None),
        P(SP_TP, None),
        P(SP, None, "tp"),
        P(SP, None, "tp"),
        P(SP, None, "tp"),
        P(),
        P(),
    )
    return jax.shard_map(shards, mesh=mesh, in_specs=placed, out_specs=P(SP_TP, None), check_vma=False)
```
